32 devices in a mesh: ep: 8 (over z, x), tp: 4 (over y, core).
Axes of the slice: x: 2, y: 2, z: 4, core: 2. Of those that a mesh axis runs over, the one named last changes fastest.
Arguments:
- queries: bfloat16 [4096, 1024], P('ep', 'tp'), may hold values from -6 to 6
- sequence_keys: bfloat16 [4096, 1024], P('ep', 'tp'), may hold values from -6 to 6
- stream_content_vectors: bfloat16 [4096, 2048], P('ep', 'tp'), may hold values from -6 to 6
- output_gate_logits: bfloat16 [4096, 2048], P('ep', 'tp'), may hold values from -6 to 6
- retention_preactivation: bfloat16 [4096, 1024], P('ep', 'tp'), may hold values from -3 to 10
- additional_fade_bias: float32 [4096, 1024], P('ep', 'tp'), may hold values from -2.1 to 0
- attention_group_rescale: float32 [128], replicated, may hold values from 0.1 to 1.9
- output_projection: bfloat16 [2048, 2048], P(None, 'tp'), may hold values from -0.125 to 0.125
- expert_batch_tokens: bfloat16 [1024, 2048], P('ep'), may hold values from -6 to 6
- expert_norm_gain: float32 [2048], replicated, may hold values from 0.1 to 1.9
- routed_expert_index: int32 [1024, 4], P('ep'), may hold values from 0 to 7, all different within a row; in each aligned block of 128 rows (0 to 127, 128 to 255, ...) at most 128 rows name the same one
- routed_expert_weights: float32 [1024, 4], P('ep'), may hold values from 0.2 to 1.2
- expert_gate_matrix: bfloat16 [8, 2048, 2048], P('ep', None, 'tp'), may hold values from -0.125 to 0.125
- expert_up_matrix: bfloat16 [8, 2048, 2048], P('ep', None, 'tp'), may hold values from -0.125 to 0.125
- expert_down_matrix: bfloat16 [8, 2048, 2048], P('ep', None, 'tp'), may hold values from -0.125 to 0.125
- shared_gate_matrix: bfloat16 [2048, 2048], P(None, 'tp'), may hold values from -0.125 to 0.125
- shared_up_matrix: bfloat16 [2048, 2048], P(None, 'tp'), may hold values from -0.125 to 0.125
- shared_down_matrix: bfloat16 [2048, 2048], P(None, 'tp'), may hold values from -0.125 to 0.125
Outputs:
- mixer_out: bfloat16 [4096, 2048], P('ep', 'tp')
- specialist_blend: bfloat16 [1024, 2048], P('ep', 'tp')
The draws below stay inside these ranges and needn't reach their ends.
Inputs may be any that keep to these rules, and one draw needn't show every extreme that they name: `routed_expert_index`: each row names 4 different experts; among the rows of one index of ep no expert is named by more than 128 rows, a bound that some block reaches.
All inputs are finite; a program needn't handle non-finite values.
Results may differ from the reference program's by a relative error of at most 0.0069.
Values may be sent and summed in bfloat16 or wider, within the bound.
A program may use at most 64 MiB of HBM per device.

```python
import math
import jax
import jax.numpy as jnp
import numpy as np
from jax import lax

D = 2048
HEADS = 16
DK = 64
DV = 128
FF = 2048
SF = 2048
TOPK = 4
BLOCK = 64
SEQ_DEV = 512
TOK_B = 128
MIX = 2048
KW = 1024
TOKENS_A = 4096
TOKENS_B = 1024
EXPERTS = 8
CAP = 128
N_EP = 8


def draw_retention_preactivation(key, part):
    kind_key, fast_key, shift_key, noise_key = jax.random.split(jax.random.fold_in(key, 11), 4)
    slow_share = 0.5
    noise = jnp.clip(jax.random.normal(noise_key, (TOKENS_A, KW), jnp.float32) * 0.5, -1.5, 1.5)
    slow = jax.random.uniform(kind_key, (KW,), jnp.float32) < slow_share
    fast_base = jax.random.uniform(fast_key, (KW,), jnp.float32, -0.5, 1.0)
    slow_base = jnp.log(jnp.float32(TOKENS_A) / 8.0)
    base = jnp.where(slow, slow_base, fast_base)
    shift = jax.random.uniform(shift_key, (TOKENS_A // SEQ_DEV, 1), jnp.float32, -0.7, 0.7)
    shift = jnp.repeat(shift, SEQ_DEV, axis=0)
    return (base[None, :] + shift + noise).astype(jnp.bfloat16)


def draw_additional_fade_bias(key, part):
    place_key, depth_key = jax.random.split(jax.random.fold_in(key, 23))
    spots = jax.random.randint(place_key, (3,), 0, TOKENS_A)
    depth = jnp.log(jax.random.uniform(depth_key, (3, KW), jnp.float32, 0.5, 0.8))
    marks = (jnp.arange(TOKENS_A)[:, None] == spots[None, :]).astype(jnp.float32)
    return jnp.dot(marks, depth, precision=jax.lax.Precision.HIGHEST)


def block_levels(stream_key, dims, shards, least, top_value):
    loudness = 1.0
    for position, shards_of in shards:
        steps = jax.random.uniform(jax.random.fold_in(jax.random.fold_in(stream_key, 6), position), (shards_of,), jnp.float32, least / len(shards), top_value / len(shards))
        loudness = loudness * jnp.repeat(jnp.exp(steps), dims[position] // shards_of).reshape((-1,) + (1,) * (len(dims) - 1 - position))
    return loudness


def routed_block(own_key, own, number, rows, count, top, limit, skew):
    order = jax.random.permutation(own_key, count)
    crowded, ordinary = portions_of(count, rows * top, limit, skew, True), portions_of(count, rows * top, limit, skew, False)
    places = jnp.arange(count)

    def named(lengths, rotation):
        used = int((lengths > 0).sum())
        fixed = max(1, used // 4)
        shifted = fixed + (places - fixed + rotation * (used - fixed)) % max(1, count - fixed)
        return jnp.zeros((count,), jnp.int32).at[order[jnp.where(places < fixed, places, shifted)]].set(jnp.asarray(lengths, jnp.int32))

    lengths = jnp.where(number % 4 == 0, named(crowded, number // 4), named(ordinary, number - number // 4 - 1))
    mixed = jax.random.permutation(jax.random.fold_in(own, 3), count)
    giver, taker = mixed[0:count // 2 * 2:2], mixed[1:count // 2 * 2:2]
    room = jnp.minimum(lengths[giver] - 1, limit - lengths[taker]) // 2
    room = jnp.where((giver == order[0]) | (taker == order[0]) | (lengths[taker] == 0), 0, jnp.maximum(room, 0))
    shifted = jax.random.randint(jax.random.fold_in(own, 4), (count // 2,), 0, 1 << 20) % (room + 1)
    lengths = lengths.at[giver].add(-shifted).at[taker].add(shifted)
    members = jnp.searchsorted(jnp.cumsum(lengths), jnp.arange(rows * top), side="right").astype(jnp.int32)
    listing = members.reshape(top, rows).T
    listing = listing[jax.random.permutation(jax.random.fold_in(own, 1), rows)]
    rotation = jax.random.randint(jax.random.fold_in(own, 2), (rows, 1), 0, top)
    return jnp.take_along_axis(listing, (jnp.arange(top)[None, :] + rotation) % top, axis=1)


def portions_of(number_of, total, limit, slope, full):
    weights = [(1 << 20) // math.isqrt(standing ** slope) + 1 for standing in range(1, number_of + 1)]
    largest = limit if full else min(limit, max(-(-total // number_of), total * weights[0] // sum(weights)))
    least = 1 if total - largest >= number_of - 1 else 0
    given, rest = [largest] + [least] * (number_of - 1), total - largest - least * (number_of - 1)
    while rest > 0:
        candidates = [i for i in range(1, number_of) if given[i] < largest] or [i for i in range(1, number_of) if given[i] < limit]
        pool, budget = sum([weights[i] for i in candidates]), rest
        for i in candidates:
            addition = min(limit - given[i], max(1, budget * weights[i] // pool), rest)
            given[i] = given[i] + addition
            rest = rest - addition
    return np.array(given)


def scatter_about(own_key, dims, scale, most, shards=(), held_as=jnp.bfloat16):
    values = scale * jax.random.normal(own_key, dims, jnp.float32)
    if shards:
        values = values * block_levels(own_key, dims, shards, -0.22, 0.18)
    return jnp.clip(values, -most, most).astype(held_as)


def setup_inputs(seed: int = 0) -> dict:
    splits = jax.random.split(jax.random.key(seed), 19)
    queries = scatter_about(splits[0], (TOKENS_A, KW), 1.0, 6.0, ((0, 8), (1, 4)))
    sequence_keys = scatter_about(splits[1], (TOKENS_A, KW), 1.0, 6.0, ((0, 8), (1, 4)))
    stream_content_vectors = scatter_about(splits[2], (TOKENS_A, MIX), 1.0, 6.0, ((0, 8), (1, 4)))
    output_gate_logits = scatter_about(splits[3], (TOKENS_A, MIX), 1.0, 6.0, ((0, 8), (1, 4)))
    retention_preactivation = draw_retention_preactivation(jax.random.fold_in(splits[18], 71), 0)
    additional_fade_bias = draw_additional_fade_bias(jax.random.fold_in(splits[18], 71), 0)
    attention_group_rescale = jnp.clip(1.0 + 0.18 * jax.random.normal(splits[6], (DV,), jnp.float32), 0.1, 1.9)
    output_projection = scatter_about(splits[7], (MIX, D), MIX ** -0.5, 0.125, ((1, 4),))
    expert_batch_tokens = scatter_about(splits[8], (TOKENS_B, D), 1.0, 6.0, ((0, 8),))
    expert_norm_gain = jnp.clip(1.0 + 0.18 * jax.random.normal(splits[9], (D,), jnp.float32), 0.1, 1.9)
    routed_expert_index_keys = jax.random.split(jax.random.fold_in(splits[10], 1), TOKENS_B // TOK_B)
    routed_expert_index_turns = jax.random.permutation(jax.random.fold_in(splits[10], 3), TOKENS_B // TOK_B)
    routed_expert_index = jax.vmap(lambda own, number: routed_block(jax.random.fold_in(splits[10], 2), own, number, TOK_B, EXPERTS, TOPK, CAP, 2))(routed_expert_index_keys, routed_expert_index_turns).reshape((TOKENS_B, TOPK))
    routed_expert_weights = jnp.clip(0.2 + 1 * jax.random.uniform(splits[11], (TOKENS_B, TOPK), jnp.float32) ** block_levels(splits[11], (TOKENS_B, TOPK), ((0, 8),), -0.2, 0.2), 0.2, 1.2)
    expert_gate_matrix = scatter_about(splits[12], (EXPERTS, D, FF), D ** -0.5, 0.125, ((0, 8), (2, 4)))
    expert_up_matrix = scatter_about(splits[13], (EXPERTS, D, FF), D ** -0.5, 0.125, ((0, 8), (2, 4)))
    expert_down_matrix = scatter_about(splits[14], (EXPERTS, FF, D), FF ** -0.5, 0.125, ((0, 8), (2, 4)))
    shared_gate_matrix = scatter_about(splits[15], (D, SF), D ** -0.5, 0.125, ((1, 4),))
    shared_up_matrix = scatter_about(splits[16], (D, SF), D ** -0.5, 0.125, ((1, 4),))
    shared_down_matrix = scatter_about(splits[17], (SF, D), SF ** -0.5, 0.125, ((1, 4),))
    return {"queries": queries, "sequence_keys": sequence_keys, "stream_content_vectors": stream_content_vectors, "output_gate_logits": output_gate_logits, "retention_preactivation": retention_preactivation, "additional_fade_bias": additional_fade_bias, "attention_group_rescale": attention_group_rescale, "output_projection": output_projection, "expert_batch_tokens": expert_batch_tokens, "expert_norm_gain": expert_norm_gain, "routed_expert_index": routed_expert_index, "routed_expert_weights": routed_expert_weights, "expert_gate_matrix": expert_gate_matrix, "expert_up_matrix": expert_up_matrix, "expert_down_matrix": expert_down_matrix, "shared_gate_matrix": shared_gate_matrix, "shared_up_matrix": shared_up_matrix, "shared_down_matrix": shared_down_matrix}


eps_norm = 1e-06
switch_softness = 16.0
highest = lax.Precision.HIGHEST

def by_head(array, blocks, width):
    heads_here = array.shape[1] // width
    return array.astype(jnp.float32).reshape(blocks, BLOCK, heads_here, width).transpose(2, 0, 1, 3)

def carry_step(state, inputs):
    decay, update = inputs
    return (decay[..., None] * state + update, state)

def reference(queries, sequence_keys, stream_content_vectors, output_gate_logits, retention_preactivation, additional_fade_bias, attention_group_rescale, output_projection, expert_batch_tokens, expert_norm_gain, routed_expert_index, routed_expert_weights, expert_gate_matrix, expert_up_matrix, expert_down_matrix, shared_gate_matrix, shared_up_matrix, shared_down_matrix):
    blocks = TOKENS_A // BLOCK
    fade_exponent_rate = jax.nn.log_sigmoid(retention_preactivation.astype(jnp.float32)) / switch_softness + additional_fade_bias
    fade_exponent_rate = by_head(fade_exponent_rate, blocks, DK)
    inner = jnp.cumsum(fade_exponent_rate, axis=2)
    last = inner[:, :, -1:, :]
    query_f = by_head(queries, blocks, DK) * DK ** (-0.5)
    key_f = by_head(sequence_keys, blocks, DK)
    value_f = by_head(stream_content_vectors, blocks, DV)
    incoming_question = query_f * jnp.exp(inner)
    key_in = key_f * jnp.exp(-inner)
    causal = jnp.tril(jnp.ones((BLOCK, BLOCK), dtype=bool))
    scores = jnp.where(causal, jnp.einsum('hnid,hnjd->hnij', incoming_question, key_in, precision=highest), 0.0)
    mixed = jnp.einsum('hnij,hnje->hnie', scores, value_f, precision=highest)
    block_kv = jnp.einsum('hncd,hnce->hnde', key_f * jnp.exp(last - inner), value_f, precision=highest)
    block_decay = jnp.exp(last[:, :, 0, :])
    start_state = jnp.zeros((HEADS, DK, DV), jnp.float32)
    final_state, entering = lax.scan(carry_step, start_state, (jnp.moveaxis(block_decay, 1, 0), jnp.moveaxis(block_kv, 1, 0)))
    entering = jnp.moveaxis(entering, 0, 1)
    mixed = mixed + jnp.einsum('hncd,hnde->hnce', incoming_question, entering, precision=highest)
    mixed = mixed.transpose(1, 2, 0, 3).reshape(TOKENS_A, HEADS, DV)
    scale = lax.rsqrt(lax.optimization_barrier(jnp.mean(mixed * mixed, axis=-1, keepdims=True)) + eps_norm)
    gate_f = jax.nn.silu(output_gate_logits.astype(jnp.float32)).reshape(TOKENS_A, HEADS, DV)
    head_out = (mixed * scale * attention_group_rescale * gate_f).reshape(TOKENS_A, MIX).astype(jnp.bfloat16)
    mixer_out = jnp.dot(head_out, output_projection, preferred_element_type=jnp.float32).astype(jnp.bfloat16)
    flat = expert_batch_tokens.astype(jnp.float32)
    normed = (flat * lax.rsqrt(lax.optimization_barrier(jnp.mean(flat * flat, axis=-1, keepdims=True)) + eps_norm) * expert_norm_gain).astype(jnp.bfloat16)
    grouped = routed_expert_index.reshape(N_EP, TOK_B * TOPK)
    expert_ids = jnp.arange(EXPERTS, dtype=jnp.int32)
    onehot = (grouped[:, :, None] == expert_ids[None, None, :]).astype(jnp.int32)
    before = jnp.cumsum(onehot, axis=1).astype(jnp.int32) - onehot
    slot = lax.optimization_barrier(jnp.sum(before * onehot, axis=2)).astype(jnp.int32)
    source = jnp.broadcast_to(jnp.arange(N_EP, dtype=jnp.int32)[:, None], grouped.shape)
    owner = source * TOK_B + (jnp.arange(TOK_B * TOPK, dtype=jnp.int32) // TOPK)[None, :]
    table = jnp.full((EXPERTS, N_EP, CAP), TOKENS_B, dtype=jnp.int32).at[grouped, source, slot].set(owner)
    padded = jnp.concatenate([normed, jnp.zeros((1, D), jnp.bfloat16)], axis=0)

    def one_expert(inputs):
        slots, gate_w, up_w, down_w = inputs
        rows = padded[slots.reshape(-1)]
        gate_part = jnp.dot(rows, gate_w, preferred_element_type=jnp.float32)
        up_part = jnp.dot(rows, up_w, preferred_element_type=jnp.float32)
        hidden = (jax.nn.silu(gate_part) * up_part).astype(jnp.bfloat16)
        result = jnp.dot(hidden, down_w, preferred_element_type=jnp.float32).astype(jnp.bfloat16)
        return result.reshape(N_EP, CAP, D)
    results = lax.map(one_expert, (table, expert_gate_matrix, expert_up_matrix, expert_down_matrix))
    picked = results[grouped, source, slot].reshape(TOKENS_B, TOPK, D).astype(jnp.float32)
    routed = lax.optimization_barrier(jnp.sum(picked * routed_expert_weights[:, :, None], axis=1))
    shared_gate_part = jnp.dot(normed, shared_gate_matrix, preferred_element_type=jnp.float32)
    shared_up_part = jnp.dot(normed, shared_up_matrix, preferred_element_type=jnp.float32)
    shared_hidden = (jax.nn.silu(shared_gate_part) * shared_up_part).astype(jnp.bfloat16)
    shared_out = jnp.dot(shared_hidden, shared_down_matrix, preferred_element_type=jnp.float32)
    specialist_blend = (shared_out + routed).astype(jnp.bfloat16)
    return (mixer_out, specialist_blend)
```

```python
import functools
import math

import jax
import jax.numpy as jnp
from jax import lax
from jax.experimental import pallas as pl
from jax.experimental.pallas import tpu as pltpu
from jax.sharding import PartitionSpec as P

DK = 64
DV = 128
BLOCK = 64
PAD = 16
CORES = 2

eps_norm = 1e-06
switch_softness = 16.0
bf16 = jnp.bfloat16
f32 = jnp.float32
NT = (((1,), (1,)), ((), ()))
TN = (((0,), (0,)), ((), ()))
MESH = pl.DeviceIdType.MESH


def silu(x):
    return x * jax.nn.sigmoid(x)


def dot(a, b):
    return jnp.dot(a, b, preferred_element_type=f32)


def body(sizes, *refs):
    Z, X, Y = sizes
    E, TP = Z * X, Y * CORES
    (
        q_hbm, k_hbm, v_hbm, og_hbm, r_hbm, b_hbm, gain_hbm, wo_hbm, tok_hbm, ng_hbm, idx_hbm, w_hbm,
        eg_hbm, eu_hbm, ed_hbm, sg_hbm, su_hbm, sd_hbm,
        mixer_hbm, blend_hbm,
        q_ref, k_ref, v_ref, og_ref, r_ref, b_ref, gain_ref, wo_ref, tok_ref, ng_ref, idx_ref, w_ref,
        eg_ref, eu_ref, ed_ref, sg_ref, su_ref, sd_ref,
        mixer_ref, blend_ref,
        R, G, RO, RI, A, B, mixed_ref, far_ref, state_ref, enter_ref, acc_ref,
        in_sem, out_sem,
        r_part_s, r_up_s, r_down_s, r_x_s, r_far_r, r_part_r,
        u_part_s, u_part_r, u_y_s, u_y_r, u_f_s, u_f_r,
        res_s, res_r, a_s, a_r, b_s, b_r,
    ) = refs

    ep, tp = lax.axis_index("ep"), lax.axis_index("tp")
    z, x = ep // X, ep % X
    y, c = tp // CORES, tp % CORES
    partner = y * CORES + (1 - c)
    rows = tok_ref.shape[0]
    half = rows // CORES
    seq, kw = q_ref.shape
    heads = kw // DK
    chunks = seq // rows
    width = G.shape[-1]

    def remote(src, dst, ssem, rsem, e, t):
        return pltpu.make_async_remote_copy(
            src_ref=src,
            dst_ref=dst,
            send_sem=ssem,
            recv_sem=rsem,
            device_id={"ep": e, "tp": t},
            device_id_type=MESH,
        )

    loads = [
        (tok_hbm, tok_ref), (ng_hbm, ng_ref), (sg_hbm, sg_ref), (su_hbm, su_ref), (eg_hbm, eg_ref), (eu_hbm, eu_ref),
        (r_hbm, r_ref), (b_hbm, b_ref), (q_hbm, q_ref), (k_hbm, k_ref), (v_hbm, v_ref),
        (sd_hbm, sd_ref), (ed_hbm, ed_ref), (og_hbm, og_ref), (gain_hbm, gain_ref), (wo_hbm, wo_ref),
        (idx_hbm, idx_ref), (w_hbm, w_ref),
    ]
    copies = {
        id(dst): pltpu.make_async_copy(src, dst, in_sem.at[n]) for n, (src, dst) in enumerate(loads)
    }
    for _, dst in loads:
        copies[id(dst)].start()

    def need(*dsts):
        for dst in dsts:
            copies[id(dst)].wait()

    barrier = pltpu.get_barrier_semaphore()
    pl.semaphore_signal(barrier, inc=1, device_id={"ep": ep, "tp": partner}, device_id_type=MESH)
    for dy in range(1, Y):
        pl.semaphore_signal(
            barrier, inc=1, device_id={"ep": ep, "tp": (y + dy) % Y * CORES + c}, device_id_type=MESH
        )
    for d in range(1, E):
        pl.semaphore_signal(
            barrier, inc=1, device_id={"ep": (ep + d) % E, "tp": tp}, device_id_type=MESH
        )

    need(tok_ref, ng_ref)
    flat = tok_ref[...].astype(f32)
    normed = (
        flat * lax.rsqrt(jnp.mean(flat * flat, axis=-1, keepdims=True) + eps_norm) * ng_ref[...]
    ).astype(bf16)
    R[ep, 0] = normed[:half]
    R[ep, 1] = normed[half:]

    pl.semaphore_wait(barrier, 1 + (Y - 1) + (E - 1))

    def row_part(b):
        return remote(R.at[b, c], R.at[b, c], r_part_s.at[b], r_part_r.at[b], ep, partner)

    def row_up(b):
        return remote(R.at[b, c], R.at[b, c], r_up_s.at[b], r_far_r.at[b], ep + X, tp)

    def row_down(b):
        return remote(R.at[b, c], R.at[b, c], r_down_s.at[b], r_far_r.at[b], ep - X, tp)

    def row_x(b, dx):
        return remote(
            R.at[b, c], R.at[b, c], r_x_s.at[dx - 1, b], r_far_r.at[b], z * X + (x + dx) % X, tp
        )

    def near(j):
        lo, hi = z, Z - 1 - z
        m = jnp.minimum(lo, hi)
        d = (j + 1) // 2
        alt = z - d if j % 2 else z + d
        return jnp.where(j <= 2 * m, alt, jnp.where(lo < hi, j, Z - 1 - j))

    def goes_up(zj):
        return (zj <= z) & (z < Z - 1)

    def goes_down(zj):
        return (zj >= z) & (z > 0)

    def send_own():
        pl.when(goes_up(z))(lambda: row_up(ep).start())
        pl.when(goes_down(z))(lambda: row_down(ep).start())
        for dx in range(1, X):
            row_x(ep, dx).start()

    def arrive(b):
        remote(R.at[b, c], R.at[b, c], r_part_s.at[b], r_far_r.at[b], ep, partner).wait_recv()

    def relay_line(j):
        zj = near(j)
        b = zj * X + x
        arrive(b)
        pl.when(goes_up(zj))(lambda: row_up(b).start())
        pl.when(goes_down(zj))(lambda: row_down(b).start())
        for dx in range(1, X):
            row_x(b, dx).start()
        row_part(b).start()

    def relay_side(j, dx):
        b = near(j) * X + (x + dx) % X
        arrive(b)
        row_part(b).start()

    def rows_of(b):
        return jnp.concatenate([R[b, 0], R[b, 1]], axis=0)

    def unit_part(u):
        return remote(G.at[u, tp], G.at[u, tp], u_part_s.at[u], u_part_r.at[u], ep, partner)

    def unit_y(u, dy):
        return remote(
            G.at[u, tp], G.at[u, tp], u_y_s.at[dy - 1, u], u_y_r.at[dy - 1, u], ep, (y + dy) % Y * CORES + c
        )

    def unit_f(u, dy):
        t = (y - dy + Y) % Y * CORES + c
        return remote(G.at[u, t], G.at[u, t], u_f_s.at[dy - 1, u], u_f_r.at[dy - 1, u], ep, partner)

    def unit_send(u):
        for dy in range(1, Y):
            unit_y(u, dy).start()
        unit_part(u).start()

    def unit_forward(u):
        for dy in range(1, Y):
            unit_y(u, dy).wait_recv()
            unit_f(u, dy).start()

    def unit_wait(u):
        unit_part(u).wait_recv()
        for dy in range(1, Y):
            unit_f(u, dy).wait_recv()

    def unit_rows(u):
        return jnp.concatenate([G[u, t] for t in range(TP)], axis=1)

    tile = min(256, width)

    def hidden(a, gate_w, up_w, units):
        def turn(n, carry):
            at = pl.ds(pl.multiple_of(n * tile, tile), tile)
            h = (silu(dot(a, gate_w[:, at])) * dot(a, up_w[:, at])).astype(bf16)
            for i, u in enumerate(units):
                G[u, tp, :, at] = h[i * rows : (i + 1) * rows]
            return carry

        lax.fori_loop(0, width // tile, turn, 0)

    def result(i, b):
        return remote(RO.at[i], RI.at[ep], res_s.at[i], res_r.at[ep], b, tp)

    row = lax.broadcasted_iota(jnp.int32, (BLOCK, BLOCK), 0)
    col = lax.broadcasted_iota(jnp.int32, (BLOCK, BLOCK), 1)
    causal = row >= col
    tril = causal.astype(f32)

    def scan_turn(n, _):
        at = pl.ds(pl.multiple_of(n * BLOCK, BLOCK), BLOCK)
        r = r_ref[at, :].astype(f32)
        log_sig = jnp.minimum(r, 0.0) - jnp.log1p(jnp.exp(-jnp.abs(r)))
        rate = log_sig / switch_softness + b_ref[at, :]
        inner = jnp.dot(tril, rate, precision=lax.Precision.HIGHEST, preferred_element_type=f32)
        last = inner[BLOCK - 1 : BLOCK, :]
        q = q_ref[at, :].astype(f32) * DK**-0.5
        k = k_ref[at, :].astype(f32)
        q_in = q * jnp.exp(inner)
        q_b = q_in.astype(bf16)
        k_b = (k * jnp.exp(-inner)).astype(bf16)
        k_out = (k * jnp.exp(last - inner)).astype(bf16)
        prior = state_ref[DV : DV + 1, :]
        far_ref[at, :] = (q * jnp.exp(inner + prior)).astype(bf16)
        entering = state_ref[0:DV, :]
        entering_b = entering.astype(bf16)
        updates = []
        for h in range(heads):
            ks = slice(h * DK, (h + 1) * DK)
            vs = slice(h * DV, (h + 1) * DV)
            v = v_ref[at, vs]
            scores = lax.dot_general(q_b[:, ks], k_b[:, ks], NT, preferred_element_type=f32)
            scores = jnp.where(causal, scores, 0.0).astype(bf16)
            out = jnp.dot(scores, v, preferred_element_type=f32)
            out += lax.dot_general(q_b[:, ks], entering_b[:, ks], NT, preferred_element_type=f32)
            mixed_ref[at, vs] = out
            updates.append(lax.dot_general(v, k_out[:, ks], TN, preferred_element_type=f32))
        state_ref[0:DV, :] = entering * jnp.exp(last) + jnp.concatenate(updates, axis=1)
        state_ref[DV : DV + 1, :] = prior + last
        return 0

    def put_state(dst, n):
        fade = state_ref[DV : DV + 8, :]
        high = fade.astype(bf16)
        low = (fade - high.astype(f32)).astype(bf16)
        dst[n, 0:DV, :] = state_ref[0:DV, :].astype(bf16)
        dst[n, DV : DV + PAD, :] = jnp.concatenate([high, low], axis=0)

    def state_a(dx):
        return remote(A.at[x], A.at[x], a_s.at[dx - 1], a_r.at[dx - 1], z * X + (x + dx) % X, tp)

    def state_b(dz):
        return remote(B.at[z], B.at[z], b_s.at[dz - 1], b_r.at[dz - 1], (ep + dz * X) % E, tp)

    def fold(src, n, state):
        fade = src[n, DV : DV + PAD, :].astype(f32)
        fade = fade[0:8] + fade[8:16]
        return fade, jnp.exp(fade[0:1]) * state + src[n, 0:DV, :].astype(f32)

    def combine():
        for dx in range(1, X):
            state_a(dx).wait_recv()
        state = jnp.zeros((DV, kw), f32)
        total = jnp.zeros((8, kw), f32)
        for n in range(X):
            fade, state = fold(A, n, state)
            total += fade
        state_ref[0:DV, :] = state
        state_ref[DV : DV + 8, :] = total
        put_state(B, z)
        for dz in range(1, Z):
            pl.when(z + dz < Z)(lambda dz=dz: state_b(dz).start())

    def enter():
        enter_ref[...] = jnp.zeros_like(enter_ref)
        for dz in range(Z - 1, 0, -1):

            @pl.when(z >= dz)
            def _(dz=dz):
                state_b(dz).wait_recv()
                enter_ref[...] = fold(B, z - dz, enter_ref[...])[1]

        for n in range(X - 1):
            state = enter_ref[...]
            enter_ref[...] = jnp.where(n < x, fold(A, n, state)[1], state)

    def finish(i):
        at = pl.ds(i * rows, rows)
        state = enter_ref[...].astype(bf16)
        gain = gain_ref[...]
        for h in range(heads):
            ks = slice(h * DK, (h + 1) * DK)
            vs = slice(h * DV, (h + 1) * DV)
            m = mixed_ref[at, vs] + lax.dot_general(
                far_ref[at, ks], state[:, ks], NT, preferred_element_type=f32
            )
            scale = lax.rsqrt(jnp.mean(m * m, axis=-1, keepdims=True) + eps_norm)
            gate = silu(og_ref[at, vs].astype(f32))
            G[1 + E + i, tp, :, vs] = (m * scale * gain * gate).astype(bf16)

    order = [(0, ep)]
    order += [(1 + n, z * X + (x + dx) % X) for n, dx in enumerate(range(1, X))]
    for j in range(1, Z):
        order += [(j * X, near(j) * X + x)]
        order += [(j * X + dx, near(j) * X + (x + dx) % X) for dx in range(1, X)]

    def expert_hidden(places):
        for n in places:
            row_part(order[n][1]).wait_recv()
        a = jnp.concatenate([rows_of(order[n][1]) for n in places], axis=0)
        hidden(a, eg_ref, eu_ref, [1 + n for n in places])
        for n in places:
            unit_send(1 + n)

    def expert_result(places):
        for n in places:
            unit_wait(1 + n)
        a = jnp.concatenate([unit_rows(1 + n) for n in places], axis=0)
        out = dot(a, ed_ref[...]).astype(bf16)
        for i, n in enumerate(places):
            RO[n] = out[i * rows : (i + 1) * rows]
        for n in places:
            if n:
                result(n, order[n][1]).start()

    turns = seq // BLOCK
    early = turns // 2

    send_own()
    own = rows_of(ep)
    need(sg_ref, su_ref)
    hidden(own, sg_ref, su_ref, [0])
    unit_send(0)
    need(eg_ref, eu_ref)
    hidden(own, eg_ref, eu_ref, [1])
    unit_send(1)
    need(r_ref, b_ref, q_ref, k_ref, v_ref)
    state_ref[...] = jnp.zeros_like(state_ref)
    lax.fori_loop(0, early, scan_turn, 0)
    unit_forward(0)
    unit_forward(1)
    pending = []
    for j in range(1, Z):
        for dx in range(1, X):
            relay_side(j - 1, dx)
        relay_line(j)
        places = [(j - 1) * X + dx for dx in range(1, X)] + [j * X]
        expert_hidden(places)
        if j == 1:
            lax.fori_loop(early, turns, scan_turn, 0)
            put_state(A, x)
            for dx in range(1, X):
                state_a(dx).start()
            need(sd_ref)
            unit_wait(0)
            acc_ref[...] = dot(unit_rows(0), sd_ref[...])
            need(ed_ref)
            for n in places:
                unit_forward(1 + n)
            expert_result([0])
            combine()
        if pending:
            expert_result(pending)
        if j > 1:
            for n in places:
                unit_forward(1 + n)
        pending = places
    need(og_ref, gain_ref)
    enter()
    for i in range(chunks):
        finish(i)
    last_places = []
    if X > 1:
        for dx in range(1, X):
            relay_side(Z - 1, dx)
            last_places.append((Z - 1) * X + dx)
        expert_hidden(last_places)
    for i in range(chunks):
        unit_send(1 + E + i)
    if pending:
        expert_result(pending)
    for n in last_places:
        unit_forward(1 + n)
    if last_places:
        expert_result(last_places)
    need(wo_ref)

    need(idx_ref, w_ref)

    def weight(e):
        return jnp.sum(jnp.where(idx_ref[...] == e, w_ref[...], 0.0), axis=1, keepdims=True)

    def mixer_out(i):
        at = pl.ds(i * rows, rows)
        return pltpu.make_async_copy(mixer_ref.at[at], mixer_hbm.at[at], out_sem.at[i])

    for i in range(chunks):
        unit_forward(1 + E + i)
        unit_wait(1 + E + i)
        mixer_ref[pl.ds(i * rows, rows), :] = dot(unit_rows(1 + E + i), wo_ref[...]).astype(bf16)
        mixer_out(i).start()

    acc_ref[...] += RO[0].astype(f32) * weight(ep)
    for n in range(1, E):
        e = order[n][1]
        remote(RO.at[n], RI.at[e], res_s.at[n], res_r.at[e], e, tp).wait_recv()
        acc_ref[...] += RI[e].astype(f32) * weight(e)
    blend_ref[...] = acc_ref[...].astype(bf16)
    blend_out = pltpu.make_async_copy(blend_ref, blend_hbm, out_sem.at[chunks])
    blend_out.start()

    for j in range(Z):
        zj = near(j)
        b = zj * X + x
        pl.when(goes_up(zj))(lambda b=b: row_up(b).wait_send())
        pl.when(goes_down(zj))(lambda b=b: row_down(b).wait_send())
        for dx in range(1, X):
            row_x(b, dx).wait_send()
    for n in range(1, E):
        row_part(order[n][1]).wait_send()
        result(n, order[n][1]).wait_send()
    for u in range(1 + E + chunks):
        unit_part(u).wait_send()
        for dy in range(1, Y):
            unit_y(u, dy).wait_send()
            unit_f(u, dy).wait_send()
    for dx in range(1, X):
        state_a(dx).wait_send()
    for dz in range(1, Z):
        pl.when(z + dz < Z)(lambda dz=dz: state_b(dz).wait_send())
    for i in range(chunks):
        mixer_out(i).wait()
    blend_out.wait()


def local(
    queries,
    sequence_keys,
    stream_content_vectors,
    output_gate_logits,
    retention_preactivation,
    additional_fade_bias,
    attention_group_rescale,
    output_projection,
    expert_batch_tokens,
    expert_norm_gain,
    routed_expert_index,
    routed_expert_weights,
    expert_gate_matrix,
    expert_up_matrix,
    expert_down_matrix,
    shared_gate_matrix,
    shared_up_matrix,
    shared_down_matrix,
):
    experts, lanes = lax.axis_size("ep"), lax.axis_size("tp")
    X = 2 ** (int(math.log2(experts)) // 2)
    Z, Y = experts // X, lanes // CORES
    rows, model_width = expert_batch_tokens.shape
    seq, kw = queries.shape
    vw = stream_content_vectors.shape[1]
    width = shared_gate_matrix.shape[1]
    chunks = seq // rows
    units = 1 + experts + chunks
    args = (
        queries,
        sequence_keys,
        stream_content_vectors,
        output_gate_logits,
        retention_preactivation,
        additional_fade_bias,
        attention_group_rescale.reshape(1, DV),
        output_projection,
        expert_batch_tokens,
        expert_norm_gain.reshape(1, model_width),
        routed_expert_index,
        routed_expert_weights,
        expert_gate_matrix[0],
        expert_up_matrix[0],
        expert_down_matrix[0],
        shared_gate_matrix,
        shared_up_matrix,
        shared_down_matrix,
    )
    outs = (
        jax.ShapeDtypeStruct((seq, output_projection.shape[1]), bf16),
        jax.ShapeDtypeStruct((rows, shared_down_matrix.shape[1]), bf16),
    )
    dma = lambda *shape: pltpu.SemaphoreType.DMA(shape)
    scratch = [pltpu.VMEM(a.shape, a.dtype) for a in args]
    scratch += [pltpu.VMEM(o.shape, o.dtype) for o in outs]
    scratch += [
        pltpu.VMEM((experts, CORES, rows // CORES, model_width), bf16),
        pltpu.VMEM((units, lanes, rows, width), bf16),
        pltpu.VMEM((experts, rows, outs[1].shape[1]), bf16),
        pltpu.VMEM((experts, rows, outs[1].shape[1]), bf16),
        pltpu.VMEM((X, DV + PAD, kw), bf16),
        pltpu.VMEM((Z, DV + PAD, kw), bf16),
        pltpu.VMEM((seq, vw), f32),
        pltpu.VMEM((seq, kw), bf16),
        pltpu.VMEM((DV + 8, kw), f32),
        pltpu.VMEM((DV, kw), f32),
        pltpu.VMEM((rows, outs[1].shape[1]), f32),
        dma(len(args)),
        dma(chunks + 1),
        dma(experts),
        dma(experts),
        dma(experts),
        dma(max(X - 1, 1), experts),
        dma(experts),
        dma(experts),
        dma(units),
        dma(units),
        dma(max(Y - 1, 1), units),
        dma(max(Y - 1, 1), units),
        dma(max(Y - 1, 1), units),
        dma(max(Y - 1, 1), units),
        dma(experts),
        dma(experts),
        dma(max(X - 1, 1)),
        dma(max(X - 1, 1)),
        dma(max(Z - 1, 1)),
        dma(max(Z - 1, 1)),
    ]
    return pl.pallas_call(
        functools.partial(body, (Z, X, Y)),
        out_shape=outs,
        in_specs=[pl.BlockSpec(memory_space=pl.ANY)] * len(args),
        out_specs=tuple([pl.BlockSpec(memory_space=pl.ANY)] * len(outs)),
        scratch_shapes=scratch,
        compiler_params=pltpu.CompilerParams(
            collective_id=0, has_side_effects=True, vmem_limit_bytes=66000000
        ),
        cost_estimate=pl.CostEstimate(
            flops=10**10, bytes_accessed=20 * 2**20, transcendentals=10**6
        ),
        name="step",
    )(*args)


def solution(mesh):
    in_specs = (
        P("ep", "tp"),
        P("ep", "tp"),
        P("ep", "tp"),
        P("ep", "tp"),
        P("ep", "tp"),
        P("ep", "tp"),
        P(),
        P(None, "tp"),
        P("ep", None),
        P(),
        P("ep", None),
        P("ep", None),
        P("ep", None, "tp"),
        P("ep", None, "tp"),
        P("ep", None, "tp"),
        P(None, "tp"),
        P(None, "tp"),
        P(None, "tp"),
    )
    out_specs = (P("ep", "tp"), P("ep", "tp"))
    return jax.shard_map(local, mesh=mesh, in_specs=in_specs, out_specs=out_specs, check_vma=False)
```

```python
import functools
import math

import jax
import jax.numpy as jnp
from jax import lax
from jax.experimental import pallas as pl
from jax.experimental.pallas import tpu as pltpu
from jax.sharding import PartitionSpec as P

DK = 64
DV = 128
BLOCK = 64
PAD = 16
CORES = 2

eps_norm = 1e-06
switch_softness = 16.0
bf16 = jnp.bfloat16
f32 = jnp.float32
NT = (((1,), (1,)), ((), ()))
TN = (((0,), (0,)), ((), ()))
MESH = pl.DeviceIdType.MESH


def silu(x):
    return x * jax.nn.sigmoid(x)


def dot(a, b):
    return jnp.dot(a, b, preferred_element_type=f32)


def body(sizes, *refs):
    Z, X, Y = sizes
    E, TP = Z * X, Y * CORES
    (
        q_hbm, k_hbm, v_hbm, og_hbm, r_hbm, b_hbm, gain_hbm, wo_hbm, tok_hbm, ng_hbm, idx_hbm, w_hbm,
        eg_hbm, eu_hbm, ed_hbm, sg_hbm, su_hbm, sd_hbm,
        mixer_hbm, blend_hbm,
        q_ref, k_ref, v_ref, og_ref, r_ref, b_ref, gain_ref, wo_ref, tok_ref, ng_ref, idx_ref, w_ref,
        eg_ref, eu_ref, ed_ref, sg_ref, su_ref, sd_ref,
        mixer_ref, blend_ref,
        R, G, RO, RI, A, B, mixed_ref, far_ref, state_ref, enter_ref, acc_ref,
        in_sem, out_sem,
        r_part_s, r_up_s, r_down_s, r_x_s, r_far_r, r_part_r,
        u_part_s, u_part_r, u_y_s, u_y_r, u_f_s, u_f_r,
        res_s, res_r, a_s, a_r, b_s, b_r,
    ) = refs

    ep, tp = lax.axis_index("ep"), lax.axis_index("tp")
    z, x = ep // X, ep % X
    y, c = tp // CORES, tp % CORES
    partner = y * CORES + (1 - c)
    rows = tok_ref.shape[0]
    half = rows // CORES
    seq, kw = q_ref.shape
    heads = kw // DK
    chunks = seq // rows
    width = G.shape[-1]

    def remote(src, dst, ssem, rsem, e, t):
        return pltpu.make_async_remote_copy(
            src_ref=src,
            dst_ref=dst,
            send_sem=ssem,
            recv_sem=rsem,
            device_id={"ep": e, "tp": t},
            device_id_type=MESH,
        )

    loads = [
        (tok_hbm, tok_ref), (ng_hbm, ng_ref), (sg_hbm, sg_ref), (su_hbm, su_ref), (eg_hbm, eg_ref), (eu_hbm, eu_ref),
        (r_hbm, r_ref), (b_hbm, b_ref), (q_hbm, q_ref), (k_hbm, k_ref), (v_hbm, v_ref),
        (sd_hbm, sd_ref), (ed_hbm, ed_ref), (og_hbm, og_ref), (gain_hbm, gain_ref), (wo_hbm, wo_ref),
        (idx_hbm, idx_ref), (w_hbm, w_ref),
    ]
    copies = {
        id(dst): pltpu.make_async_copy(src, dst, in_sem.at[n]) for n, (src, dst) in enumerate(loads)
    }
    for _, dst in loads:
        copies[id(dst)].start()

    def need(*dsts):
        for dst in dsts:
            copies[id(dst)].wait()

    barrier = pltpu.get_barrier_semaphore()
    pl.semaphore_signal(barrier, inc=1, device_id={"ep": ep, "tp": partner}, device_id_type=MESH)
    for dy in range(1, Y):
        pl.semaphore_signal(
            barrier, inc=1, device_id={"ep": ep, "tp": (y + dy) % Y * CORES + c}, device_id_type=MESH
        )
    for d in range(1, E):
        pl.semaphore_signal(
            barrier, inc=1, device_id={"ep": (ep + d) % E, "tp": tp}, device_id_type=MESH
        )

    with jax.named_scope("need_tok"):
        need(tok_ref, ng_ref)
    flat = tok_ref[...].astype(f32)
    normed = (
        flat * lax.rsqrt(jnp.mean(flat * flat, axis=-1, keepdims=True) + eps_norm) * ng_ref[...]
    ).astype(bf16)
    R[ep, 0] = normed[:half]
    R[ep, 1] = normed[half:]

    with jax.named_scope("barrier"):
        pl.semaphore_wait(barrier, 1 + (Y - 1) + (E - 1))

    def row_part(b):
        return remote(R.at[b, c], R.at[b, c], r_part_s.at[b], r_part_r.at[b], ep, partner)

    def row_up(b):
        return remote(R.at[b, c], R.at[b, c], r_up_s.at[b], r_far_r.at[b], ep + X, tp)

    def row_down(b):
        return remote(R.at[b, c], R.at[b, c], r_down_s.at[b], r_far_r.at[b], ep - X, tp)

    def row_x(b, dx):
        return remote(
            R.at[b, c], R.at[b, c], r_x_s.at[dx - 1, b], r_far_r.at[b], z * X + (x + dx) % X, tp
        )

    def near(j):
        lo, hi = z, Z - 1 - z
        m = jnp.minimum(lo, hi)
        d = (j + 1) // 2
        alt = z - d if j % 2 else z + d
        return jnp.where(j <= 2 * m, alt, jnp.where(lo < hi, j, Z - 1 - j))

    def goes_up(zj):
        return (zj <= z) & (z < Z - 1)

    def goes_down(zj):
        return (zj >= z) & (z > 0)

    def send_own():
        pl.when(goes_up(z))(lambda: row_up(ep).start())
        pl.when(goes_down(z))(lambda: row_down(ep).start())
        for dx in range(1, X):
            row_x(ep, dx).start()

    def arrive(b):
        remote(R.at[b, c], R.at[b, c], r_part_s.at[b], r_far_r.at[b], ep, partner).wait_recv()

    def relay_line(k):
        @pl.when(z >= k)
        def _():
            b = ep - k * X
            arrive(b)
            pl.when(z < Z - 1)(lambda: row_up(b).start())
            for dx in range(1, X):
                row_x(b, dx).start()
            row_part(b).start()

        @pl.when(z + k < Z)
        def _():
            b = ep + k * X
            arrive(b)
            pl.when(z > 0)(lambda: row_down(b).start())
            for dx in range(1, X):
                row_x(b, dx).start()
            row_part(b).start()

    def relay_side(j, dx):
        b = near(j) * X + (x + dx) % X
        arrive(b)
        row_part(b).start()

    def rows_of(b):
        return jnp.concatenate([R[b, 0], R[b, 1]], axis=0)

    def unit_part(u):
        return remote(G.at[u, tp], G.at[u, tp], u_part_s.at[u], u_part_r.at[u], ep, partner)

    def unit_y(u, dy):
        return remote(
            G.at[u, tp], G.at[u, tp], u_y_s.at[dy - 1, u], u_y_r.at[dy - 1, u], ep, (y + dy) % Y * CORES + c
        )

    def unit_f(u, dy):
        t = (y - dy + Y) % Y * CORES + c
        return remote(G.at[u, t], G.at[u, t], u_f_s.at[dy - 1, u], u_f_r.at[dy - 1, u], ep, partner)

    def unit_send(u):
        for dy in range(1, Y):
            unit_y(u, dy).start()
        unit_part(u).start()

    def unit_forward(u):
        for dy in range(1, Y):
            unit_y(u, dy).wait_recv()
            unit_f(u, dy).start()

    def unit_wait(u):
        unit_part(u).wait_recv()
        for dy in range(1, Y):
            unit_f(u, dy).wait_recv()

    def unit_rows(u):
        return jnp.concatenate([G[u, t] for t in range(TP)], axis=1)

    tile = min(256, width)

    def hidden(a, gate_w, up_w, units):
        def turn(n, carry):
            at = pl.ds(pl.multiple_of(n * tile, tile), tile)
            h = (silu(dot(a, gate_w[:, at])) * dot(a, up_w[:, at])).astype(bf16)
            for i, u in enumerate(units):
                G[u, tp, :, at] = h[i * rows : (i + 1) * rows]
            return carry

        lax.fori_loop(0, width // tile, turn, 0)

    def result(i, b):
        return remote(RO.at[i], RI.at[ep], res_s.at[i], res_r.at[ep], b, tp)

    row = lax.broadcasted_iota(jnp.int32, (BLOCK, BLOCK), 0)
    col = lax.broadcasted_iota(jnp.int32, (BLOCK, BLOCK), 1)
    causal = row >= col
    tril = causal.astype(f32)

    def scan_turn(n, _):
        at = pl.ds(pl.multiple_of(n * BLOCK, BLOCK), BLOCK)
        r = r_ref[at, :].astype(f32)
        log_sig = jnp.minimum(r, 0.0) - jnp.log1p(jnp.exp(-jnp.abs(r)))
        rate = log_sig / switch_softness + b_ref[at, :]
        inner = jnp.dot(tril, rate, precision=lax.Precision.HIGHEST, preferred_element_type=f32)
        last = inner[BLOCK - 1 : BLOCK, :]
        q = q_ref[at, :].astype(f32) * DK**-0.5
        k = k_ref[at, :].astype(f32)
        q_in = q * jnp.exp(inner)
        q_b = q_in.astype(bf16)
        k_b = (k * jnp.exp(-inner)).astype(bf16)
        k_out = (k * jnp.exp(last - inner)).astype(bf16)
        prior = state_ref[DV : DV + 1, :]
        far_ref[at, :] = (q * jnp.exp(inner + prior)).astype(bf16)
        entering = state_ref[0:DV, :]
        entering_b = entering.astype(bf16)
        updates = []
        for h in range(heads):
            ks = slice(h * DK, (h + 1) * DK)
            vs = slice(h * DV, (h + 1) * DV)
            v = v_ref[at, vs]
            scores = lax.dot_general(q_b[:, ks], k_b[:, ks], NT, preferred_element_type=f32)
            scores = jnp.where(causal, scores, 0.0).astype(bf16)
            out = jnp.dot(scores, v, preferred_element_type=f32)
            out += lax.dot_general(q_b[:, ks], entering_b[:, ks], NT, preferred_element_type=f32)
            mixed_ref[at, vs] = out
            updates.append(lax.dot_general(v, k_out[:, ks], TN, preferred_element_type=f32))
        state_ref[0:DV, :] = entering * jnp.exp(last) + jnp.concatenate(updates, axis=1)
        state_ref[DV : DV + 1, :] = prior + last
        return 0

    def put_state(dst, n):
        fade = state_ref[DV : DV + 8, :]
        high = fade.astype(bf16)
        low = (fade - high.astype(f32)).astype(bf16)
        dst[n, 0:DV, :] = state_ref[0:DV, :].astype(bf16)
        dst[n, DV : DV + PAD, :] = jnp.concatenate([high, low], axis=0)

    def state_a(dx):
        return remote(A.at[x], A.at[x], a_s.at[dx - 1], a_r.at[dx - 1], z * X + (x + dx) % X, tp)

    def state_b(dz):
        return remote(B.at[z], B.at[z], b_s.at[dz - 1], b_r.at[dz - 1], (ep + dz * X) % E, tp)

    def fold(src, n, state):
        fade = src[n, DV : DV + PAD, :].astype(f32)
        fade = fade[0:8] + fade[8:16]
        return fade, jnp.exp(fade[0:1]) * state + src[n, 0:DV, :].astype(f32)

    def combine():
        for dx in range(1, X):
            state_a(dx).wait_recv()
        state = jnp.zeros((DV, kw), f32)
        total = jnp.zeros((8, kw), f32)
        for n in range(X):
            fade, state = fold(A, n, state)
            total += fade
        state_ref[0:DV, :] = state
        state_ref[DV : DV + 8, :] = total
        put_state(B, z)
        for dz in range(1, Z):
            pl.when(z + dz < Z)(lambda dz=dz: state_b(dz).start())

    def enter():
        enter_ref[...] = jnp.zeros_like(enter_ref)
        for dz in range(Z - 1, 0, -1):

            @pl.when(z >= dz)
            def _(dz=dz):
                state_b(dz).wait_recv()
                enter_ref[...] = fold(B, z - dz, enter_ref[...])[1]

        for n in range(X - 1):
            state = enter_ref[...]
            enter_ref[...] = jnp.where(n < x, fold(A, n, state)[1], state)

    def finish(i):
        at = pl.ds(i * rows, rows)
        state = enter_ref[...].astype(bf16)
        gain = gain_ref[...]
        for h in range(heads):
            ks = slice(h * DK, (h + 1) * DK)
            vs = slice(h * DV, (h + 1) * DV)
            m = mixed_ref[at, vs] + lax.dot_general(
                far_ref[at, ks], state[:, ks], NT, preferred_element_type=f32
            )
            scale = lax.rsqrt(jnp.mean(m * m, axis=-1, keepdims=True) + eps_norm)
            gate = silu(og_ref[at, vs].astype(f32))
            G[1 + E + i, tp, :, vs] = (m * scale * gain * gate).astype(bf16)

    order = [(0, ep)]
    order += [(1 + n, z * X + (x + dx) % X) for n, dx in enumerate(range(1, X))]
    for j in range(1, Z):
        order += [(j * X, near(j) * X + x)]
        order += [(j * X + dx, near(j) * X + (x + dx) % X) for dx in range(1, X)]

    def expert_hidden(places, name):
        with jax.named_scope("rows_wait_" + name):
            for n in places:
                row_part(order[n][1]).wait_recv()
        with jax.named_scope("hidden_" + name):
            a = jnp.concatenate([rows_of(order[n][1]) for n in places], axis=0)
            hidden(a, eg_ref, eu_ref, [1 + n for n in places])
            for n in places:
                unit_send(1 + n)

    def expert_result(places, name):
        with jax.named_scope("units_wait_" + name):
            for n in places:
                unit_wait(1 + n)
        with jax.named_scope("down_" + name):
            a = jnp.concatenate([unit_rows(1 + n) for n in places], axis=0)
            out = dot(a, ed_ref[...]).astype(bf16)
            for i, n in enumerate(places):
                RO[n] = out[i * rows : (i + 1) * rows]
            for n in places:
                if n:
                    result(n, order[n][1]).start()

    turns = seq // BLOCK
    early = turns // 2

    send_own()
    own = rows_of(ep)
    with jax.named_scope("need_shared"):
        need(sg_ref, su_ref)
    with jax.named_scope("hidden_shared"):
        hidden(own, sg_ref, su_ref, [0])
        unit_send(0)
    with jax.named_scope("need_expert"):
        need(eg_ref, eu_ref)
    with jax.named_scope("hidden_own"):
        hidden(own, eg_ref, eu_ref, [1])
        unit_send(1)
    with jax.named_scope("scan_early"):
        need(r_ref, b_ref, q_ref, k_ref, v_ref)
        state_ref[...] = jnp.zeros_like(state_ref)
        lax.fori_loop(0, early, scan_turn, 0)
    with jax.named_scope("fwd01"):
        unit_forward(0)
        unit_forward(1)
    pending = []
    for j in range(1, Z):
        with jax.named_scope(f"relay{j}"):
            relay_line(j)
            for dx in range(1, X):
                relay_side(j - 1, dx)
        places = [(j - 1) * X + dx for dx in range(1, X)] + [j * X]
        expert_hidden(places, f"{j}")
        if j == 1:
            with jax.named_scope("scan_late"):
                lax.fori_loop(early, turns, scan_turn, 0)
                put_state(A, x)
                for dx in range(1, X):
                    state_a(dx).start()
            with jax.named_scope("down_shared"):
                need(sd_ref)
                unit_wait(0)
                acc_ref[...] = dot(unit_rows(0), sd_ref[...])
            need(ed_ref)
            expert_result([0], "own")
        if j == min(2, Z - 1):
            with jax.named_scope("combine"):
                combine()
        if pending:
            with jax.named_scope(f"fwd{j - 1}"):
                for n in pending:
                    unit_forward(1 + n)
            expert_result(pending, f"{j - 1}")
        pending = places
    with jax.named_scope("enter"):
        need(og_ref, gain_ref)
        enter()
    with jax.named_scope("finish"):
        for i in range(chunks):
            finish(i)
    unit_send(1 + E)
    last_places = []
    if X > 1:
        with jax.named_scope("relay_last"):
            for dx in range(1, X):
                relay_side(Z - 1, dx)
                last_places.append((Z - 1) * X + dx)
        expert_hidden(last_places, "last")
    for i in range(1, chunks):
        unit_send(1 + E + i)
    if pending:
        with jax.named_scope("fwd_pending"):
            for n in pending:
                unit_forward(1 + n)
        expert_result(pending, "pending")
    with jax.named_scope("fwd_last"):
        unit_forward(1 + E)
        for n in last_places:
            unit_forward(1 + n)
    if last_places:
        expert_result(last_places, "last")
    need(wo_ref)
    need(idx_ref, w_ref)

    index, given = idx_ref[...], w_ref[...]
    by_expert = [jnp.sum(jnp.where(index == e, given, 0.0), axis=0, keepdims=True) for e in range(E)]
    by_expert = jnp.transpose(jnp.concatenate(by_expert, axis=0), (1, 0))
    lane = lax.broadcasted_iota(jnp.int32, by_expert.shape, 1)

    def weight(e):
        return jnp.sum(jnp.where(lane == e, by_expert, 0.0), axis=1, keepdims=True)

    def mixer_out(i):
        at = pl.ds(i * rows, rows)
        return pltpu.make_async_copy(mixer_ref.at[at], mixer_hbm.at[at], out_sem.at[i])

    for i in range(chunks):
        with jax.named_scope(f"mixer_wait{i}"):
            if i:
                unit_forward(1 + E + i)
            unit_wait(1 + E + i)
        with jax.named_scope(f"mixer{i}"):
            mixer_ref[pl.ds(i * rows, rows), :] = dot(unit_rows(1 + E + i), wo_ref[...]).astype(bf16)
            mixer_out(i).start()

    with jax.named_scope("collect"):
        acc_ref[...] += RO[0].astype(f32) * weight(ep)
        for n in range(1, E):
            e = order[n][1]
            remote(RO.at[n], RI.at[e], res_s.at[n], res_r.at[e], e, tp).wait_recv()
            acc_ref[...] += RI[e].astype(f32) * weight(e)
        blend_ref[...] = acc_ref[...].astype(bf16)
        blend_out = pltpu.make_async_copy(blend_ref, blend_hbm, out_sem.at[chunks])
        blend_out.start()

    with jax.named_scope("drain"):
        for j in range(Z):
            zj = near(j)
            b = zj * X + x
            pl.when(goes_up(zj))(lambda b=b: row_up(b).wait_send())
            pl.when(goes_down(zj))(lambda b=b: row_down(b).wait_send())
            for dx in range(1, X):
                row_x(b, dx).wait_send()
        for n in range(1, E):
            row_part(order[n][1]).wait_send()
            result(n, order[n][1]).wait_send()
        for u in range(1 + E + chunks):
            unit_part(u).wait_send()
            for dy in range(1, Y):
                unit_y(u, dy).wait_send()
                unit_f(u, dy).wait_send()
        for dx in range(1, X):
            state_a(dx).wait_send()
        for dz in range(1, Z):
            pl.when(z + dz < Z)(lambda dz=dz: state_b(dz).wait_send())
        for i in range(chunks):
            mixer_out(i).wait()
        blend_out.wait()


def local(
    queries,
    sequence_keys,
    stream_content_vectors,
    output_gate_logits,
    retention_preactivation,
    additional_fade_bias,
    attention_group_rescale,
    output_projection,
    expert_batch_tokens,
    expert_norm_gain,
    routed_expert_index,
    routed_expert_weights,
    expert_gate_matrix,
    expert_up_matrix,
    expert_down_matrix,
    shared_gate_matrix,
    shared_up_matrix,
    shared_down_matrix,
):
    experts, lanes = lax.axis_size("ep"), lax.axis_size("tp")
    X = 2 ** (int(math.log2(experts)) // 2)
    Z, Y = experts // X, lanes // CORES
    rows, model_width = expert_batch_tokens.shape
    seq, kw = queries.shape
    vw = stream_content_vectors.shape[1]
    width = shared_gate_matrix.shape[1]
    chunks = seq // rows
    units = 1 + experts + chunks
    args = (
        queries,
        sequence_keys,
        stream_content_vectors,
        output_gate_logits,
        retention_preactivation,
        additional_fade_bias,
        attention_group_rescale.reshape(1, DV),
        output_projection,
        expert_batch_tokens,
        expert_norm_gain.reshape(1, model_width),
        routed_expert_index.T,
        routed_expert_weights.T,
        expert_gate_matrix[0],
        expert_up_matrix[0],
        expert_down_matrix[0],
        shared_gate_matrix,
        shared_up_matrix,
        shared_down_matrix,
    )
    outs = (
        jax.ShapeDtypeStruct((seq, output_projection.shape[1]), bf16),
        jax.ShapeDtypeStruct((rows, shared_down_matrix.shape[1]), bf16),
    )
    dma = lambda *shape: pltpu.SemaphoreType.DMA(shape)
    scratch = [pltpu.VMEM(a.shape, a.dtype) for a in args]
    scratch += [pltpu.VMEM(o.shape, o.dtype) for o in outs]
    scratch += [
        pltpu.VMEM((experts, CORES, rows // CORES, model_width), bf16),
        pltpu.VMEM((units, lanes, rows, width), bf16),
        pltpu.VMEM((experts, rows, outs[1].shape[1]), bf16),
        pltpu.VMEM((experts, rows, outs[1].shape[1]), bf16),
        pltpu.VMEM((X, DV + PAD, kw), bf16),
        pltpu.VMEM((Z, DV + PAD, kw), bf16),
        pltpu.VMEM((seq, vw), f32),
        pltpu.VMEM((seq, kw), bf16),
        pltpu.VMEM((DV + 8, kw), f32),
        pltpu.VMEM((DV, kw), f32),
        pltpu.VMEM((rows, outs[1].shape[1]), f32),
        dma(len(args)),
        dma(chunks + 1),
        dma(experts),
        dma(experts),
        dma(experts),
        dma(max(X - 1, 1), experts),
        dma(experts),
        dma(experts),
        dma(units),
        dma(units),
        dma(max(Y - 1, 1), units),
        dma(max(Y - 1, 1), units),
        dma(max(Y - 1, 1), units),
        dma(max(Y - 1, 1), units),
        dma(experts),
        dma(experts),
        dma(max(X - 1, 1)),
        dma(max(X - 1, 1)),
        dma(max(Z - 1, 1)),
        dma(max(Z - 1, 1)),
    ]
    return pl.pallas_call(
        functools.partial(body, (Z, X, Y)),
        out_shape=outs,
        in_specs=[pl.BlockSpec(memory_space=pl.ANY)] * len(args),
        out_specs=tuple([pl.BlockSpec(memory_space=pl.ANY)] * len(outs)),
        scratch_shapes=scratch,
        compiler_params=pltpu.CompilerParams(
            collective_id=0, has_side_effects=True, vmem_limit_bytes=66000000
        ),
        cost_estimate=pl.CostEstimate(
            flops=10**10, bytes_accessed=20 * 2**20, transcendentals=10**6
        ),
        name="step",
    )(*args)


def solution(mesh):
    in_specs = (
        P("ep", "tp"),
        P("ep", "tp"),
        P("ep", "tp"),
        P("ep", "tp"),
        P("ep", "tp"),
        P("ep", "tp"),
        P(),
        P(None, "tp"),
        P("ep", None),
        P(),
        P("ep", None),
        P("ep", None),
        P("ep", None, "tp"),
        P("ep", None, "tp"),
        P("ep", None, "tp"),
        P(None, "tp"),
        P(None, "tp"),
        P(None, "tp"),
    )
    out_specs = (P("ep", "tp"), P("ep", "tp"))
    return jax.shard_map(local, mesh=mesh, in_specs=in_specs, out_specs=out_specs, check_vma=False)
```

```python
import functools
import math

import jax
import jax.numpy as jnp
from jax import lax
from jax.experimental import pallas as pl
from jax.experimental.pallas import tpu as pltpu
from jax.sharding import PartitionSpec as P

DK = 64
DV = 128
BLOCK = 64
PAD = 16
CORES = 2
CH = 2

eps_norm = 1e-06
switch_softness = 16.0
bf16 = jnp.bfloat16
f32 = jnp.float32
NT = (((1,), (1,)), ((), ()))
TN = (((0,), (0,)), ((), ()))
MESH = pl.DeviceIdType.MESH


def silu(x):
    return x * jax.nn.sigmoid(x)


def dot(a, b):
    return jnp.dot(a, b, preferred_element_type=f32)


def body(sizes, *refs):
    Z, X, Y = sizes
    E, TP = Z * X, Y * CORES
    (
        q_hbm, k_hbm, v_hbm, og_hbm, r_hbm, b_hbm, gain_hbm, wo_hbm, tok_hbm, ng_hbm, idx_hbm, w_hbm,
        eg_hbm, eu_hbm, ed_hbm, sg_hbm, su_hbm, sd_hbm,
        mixer_hbm, blend_hbm,
        q_ref, k_ref, v_ref, og_ref, r_ref, b_ref, gain_ref, wo_ref, tok_ref, ng_ref, idx_ref, w_ref,
        eg_ref, eu_ref, ed_ref, sg_ref, su_ref, sd_ref,
        mixer_ref, blend_ref,
        R, GS, GE, GL, GH, RO, RI, A, B, mixed_ref, far_ref, state_ref, enter_ref, acc_ref,
        in_sem, out_sem,
        r_part_s, r_z_s, r_down_s, r_x_s, r_far_r, r_part_r,
        u_part_s, u_part_r, u_y_s, u_y_r, u_f_s, u_f_r,
        res_s, res_r, a_s, a_r, b_s, b_r,
    ) = refs

    ep, tp = lax.axis_index("ep"), lax.axis_index("tp")
    z, x = ep // X, ep % X
    y, c = tp // CORES, tp % CORES
    partner = y * CORES + (1 - c)
    rows = tok_ref.shape[0]
    seq, kw = q_ref.shape
    heads = kw // DK
    chunks = seq // rows
    width = GS.shape[-1]
    part = rows // (CH * CORES)

    def remote(src, dst, ssem, rsem, e, t):
        return pltpu.make_async_remote_copy(
            src_ref=src,
            dst_ref=dst,
            send_sem=ssem,
            recv_sem=rsem,
            device_id={"ep": e, "tp": t},
            device_id_type=MESH,
        )

    early = [
        (tok_hbm, tok_ref), (ng_hbm, ng_ref), (sg_hbm, sg_ref), (su_hbm, su_ref), (eg_hbm, eg_ref), (eu_hbm, eu_ref),
        (r_hbm, r_ref), (b_hbm, b_ref), (q_hbm, q_ref), (k_hbm, k_ref), (v_hbm, v_ref),
    ]
    late = [
        (sd_hbm, sd_ref), (ed_hbm, ed_ref), (og_hbm, og_ref), (gain_hbm, gain_ref), (wo_hbm, wo_ref),
        (idx_hbm, idx_ref), (w_hbm, w_ref),
    ]
    copies = {}

    def load(pairs):
        for n, (src, dst) in enumerate(pairs):
            copies[id(dst)] = pltpu.make_async_copy(src, dst, in_sem.at[n])
            copies[id(dst)].start()

    load(early)

    def need(*dsts):
        for dst in dsts:
            copies[id(dst)].wait()

    class Sends:
        def __init__(self, sems, count):
            self.sems, self.count, self.sent, self.held = sems, count, 0, {}

        def start(self, make):
            n = self.sent % self.count
            if n in self.held:
                self.held[n].wait_send()
            self.held[n] = make(self.sems.at[n])
            self.held[n].start()
            self.sent += 1

        def drain(self):
            for copy in self.held.values():
                copy.wait_send()

    barrier = pltpu.get_barrier_semaphore()

    def greet(e, t):
        pl.semaphore_signal(barrier, inc=1, device_id={"ep": e, "tp": t}, device_id_type=MESH)

    greet(ep, partner)
    for dy in range(1, Y):
        greet(ep, (y + dy) % Y * CORES + c)
    for dx in range(1, X):
        greet(z * X + (x + dx) % X, tp)
    pl.when(z < Z - 1)(lambda: greet(ep + X, tp))
    pl.when(z > 0)(lambda: greet(ep - X, tp))

    need(tok_ref, ng_ref)
    flat = tok_ref[...].astype(f32)
    normed = (
        flat * lax.rsqrt(jnp.mean(flat * flat, axis=-1, keepdims=True) + eps_norm) * ng_ref[...]
    ).astype(bf16)
    for n in range(CH * CORES):
        R[ep, n // CORES, n % CORES] = normed[n * part : (n + 1) * part]

    lines = jnp.where(z < Z - 1, 1, 0) + jnp.where(z > 0, 1, 0)
    pl.semaphore_wait(barrier, 1 + (Y - 1) + (X - 1) + lines)

    def row_part(b, h, kind=0):
        return remote(R.at[b, h, c], R.at[b, h, c], r_part_s.at[kind, h], r_part_r.at[b, h], ep, partner)

    def row_up(b, h):
        return remote(R.at[b, h, c], R.at[b, h, c], r_z_s.at[b // X, h], r_far_r.at[b, h], ep + X, tp)

    def row_down(b, h, sem=None):
        sem = r_z_s.at[b // X, h] if sem is None else sem
        return remote(R.at[b, h, c], R.at[b, h, c], sem, r_far_r.at[b, h], ep - X, tp)

    def row_x(b, h, dx):
        there = z * X + (x + dx) % X
        return remote(R.at[b, h, c], R.at[b, h, c], r_x_s.at[dx - 1, b // X, h], r_far_r.at[b, h], there, tp)

    def near(j):
        up = jnp.where(j <= Z - 1 - z, z + j, Z - 1 - j)
        down = jnp.where(j <= z, z - j, j)
        return jnp.where(2 * z < Z, up, down)

    def send_own(h):
        pl.when(z < Z - 1)(lambda: row_up(ep, h).start())
        pl.when(z > 0)(lambda: row_down(ep, h, r_down_s.at[h]).start())
        for dx in range(1, X):
            row_x(ep, h, dx).start()

    def arrive(b, h):
        remote(R.at[b, h, c], R.at[b, h, c], r_part_s.at[0, h], r_far_r.at[b, h], ep, partner).wait_recv()

    def hand_over(b, h, kind, again):
        copy = row_part(b, h, kind)
        if again:
            copy.wait_send()
        copy.start()

    def relay_line(k, h):
        @pl.when(z >= k)
        def _():
            b = ep - k * X
            arrive(b, h)
            pl.when(z < Z - 1)(lambda: row_up(b, h).start())
            hand_over(b, h, 0, k > 1)

        @pl.when(z + k < Z)
        def _():
            b = ep + k * X
            arrive(b, h)
            pl.when(z > 0)(lambda: row_down(b, h).start())
            hand_over(b, h, 1, k > 1)

        for dx in range(1, X):
            row_x(near(k) * X + x, h, dx).start()

    def relay_side(j, h, dx):
        b = near(j) * X + (x + dx) % X
        arrive(b, h)
        hand_over(b, h, 1 + dx, j > 0)

    def rows_of(b, h):
        return jnp.concatenate([R[b, h, n] for n in range(CORES)], axis=0)

    part_sends = Sends(u_part_s, u_part_s.shape[0])
    y_sends = [Sends(u_y_s.at[n], u_y_s.shape[1]) for n in range(Y - 1)]
    f_sends = [Sends(u_f_s.at[n], u_f_s.shape[1]) for n in range(Y - 1)]
    result_sends = Sends(res_s, res_s.shape[0])

    def unit_part(unit, sem=None):
        G, n, u = unit
        sem = u_part_s.at[0] if sem is None else sem
        return remote(G.at[n, tp], G.at[n, tp], sem, u_part_r.at[u], ep, partner)

    def unit_y(unit, dy, sem=None):
        G, n, u = unit
        t = (y + dy) % Y * CORES + c
        sem = u_y_s.at[dy - 1, 0] if sem is None else sem
        return remote(G.at[n, tp], G.at[n, tp], sem, u_y_r.at[dy - 1, u], ep, t)

    def unit_f(unit, dy, sem=None):
        G, n, u = unit
        t = (y - dy + Y) % Y * CORES + c
        sem = u_f_s.at[dy - 1, 0] if sem is None else sem
        return remote(G.at[n, t], G.at[n, t], sem, u_f_r.at[dy - 1, u], ep, partner)

    def unit_send(unit):
        for dy in range(1, Y):
            y_sends[dy - 1].start(lambda sem: unit_y(unit, dy, sem))
        part_sends.start(lambda sem: unit_part(unit, sem))

    def unit_forward(unit):
        for dy in range(1, Y):
            unit_y(unit, dy).wait_recv()
            f_sends[dy - 1].start(lambda sem: unit_f(unit, dy, sem))

    def unit_wait(unit):
        unit_part(unit).wait_recv()
        for dy in range(1, Y):
            unit_f(unit, dy).wait_recv()

    def unit_rows(unit):
        return jnp.concatenate([unit[0][unit[1], t] for t in range(TP)], axis=1)

    shared_unit, own_unit = (GS, 0, 0), (GS, 1, 1)
    stages = (Z - 1) * CH
    stage_units = [(GE, n, 2 + n) for n in range(stages)]
    last_unit = (GL, 0, 2 + stages)
    head_units = [(GH, n, 3 + stages + n) for n in range(chunks)]

    tile = min(256, width)

    def hidden(a, gate_w, up_w, unit):
        def turn(n, carry):
            at = pl.ds(pl.multiple_of(n * tile, tile), tile)
            h = silu(dot(a, gate_w[:, at])) * dot(a, up_w[:, at])
            unit[0][unit[1], tp, :, at] = h.astype(bf16)
            return carry

        lax.fori_loop(0, width // tile, turn, 0)

    def send_result(n, h):
        result_sends.start(
            lambda sem: remote(RO.at[n, h], RI.at[ep, h], sem, res_r.at[ep, h], order[n], tp)
        )

    row = lax.broadcasted_iota(jnp.int32, (BLOCK, BLOCK), 0)
    col = lax.broadcasted_iota(jnp.int32, (BLOCK, BLOCK), 1)
    causal = row >= col
    tril = causal.astype(f32)

    def scan_turn(n, _):
        at = pl.ds(pl.multiple_of(n * BLOCK, BLOCK), BLOCK)
        r = r_ref[at, :].astype(f32)
        log_sig = jnp.minimum(r, 0.0) - jnp.log1p(jnp.exp(-jnp.abs(r)))
        rate = log_sig / switch_softness + b_ref[at, :]
        inner = jnp.dot(tril, rate, precision=lax.Precision.HIGHEST, preferred_element_type=f32)
        last = inner[BLOCK - 1 : BLOCK, :]
        q = q_ref[at, :].astype(f32) * DK**-0.5
        k = k_ref[at, :].astype(f32)
        q_in = q * jnp.exp(inner)
        q_b = q_in.astype(bf16)
        k_b = (k * jnp.exp(-inner)).astype(bf16)
        k_out = (k * jnp.exp(last - inner)).astype(bf16)
        prior = state_ref[DV : DV + 1, :]
        far_ref[at, :] = (q * jnp.exp(inner + prior)).astype(bf16)
        entering = state_ref[0:DV, :]
        entering_b = entering.astype(bf16)
        updates = []
        for h in range(heads):
            ks = slice(h * DK, (h + 1) * DK)
            vs = slice(h * DV, (h + 1) * DV)
            v = v_ref[at, vs]
            scores = lax.dot_general(q_b[:, ks], k_b[:, ks], NT, preferred_element_type=f32)
            scores = jnp.where(causal, scores, 0.0).astype(bf16)
            out = jnp.dot(scores, v, preferred_element_type=f32)
            out += lax.dot_general(q_b[:, ks], entering_b[:, ks], NT, preferred_element_type=f32)
            mixed_ref[at, vs] = out
            updates.append(lax.dot_general(v, k_out[:, ks], TN, preferred_element_type=f32))
        state_ref[0:DV, :] = entering * jnp.exp(last) + jnp.concatenate(updates, axis=1)
        state_ref[DV : DV + 1, :] = prior + last
        return 0

    def put_state(dst, n):
        fade = state_ref[DV : DV + 8, :]
        high = fade.astype(bf16)
        low = (fade - high.astype(f32)).astype(bf16)
        dst[n, 0:DV, :] = state_ref[0:DV, :].astype(bf16)
        dst[n, DV : DV + PAD, :] = jnp.concatenate([high, low], axis=0)

    def state_a(dx):
        return remote(A.at[x], A.at[x], a_s.at[dx - 1], a_r.at[dx - 1], z * X + (x + dx) % X, tp)

    def state_b():
        return remote(B.at[0], B.at[1], b_s.at[0], b_r.at[0], (ep + X) % E, tp)

    def fold(src, n, state):
        fade = src[n, DV : DV + PAD, :].astype(f32)
        fade = fade[0:8] + fade[8:16]
        return fade, jnp.exp(fade[0:1]) * state + src[n, 0:DV, :].astype(f32)

    def combine():
        for dx in range(1, X):
            state_a(dx).wait_recv()
        state = jnp.zeros((DV, kw), f32)
        total = jnp.zeros((8, kw), f32)
        for n in range(X):
            fade, state = fold(A, n, state)
            total += fade
        state_ref[0:DV, :] = state
        state_ref[DV : DV + 8, :] = total
        enter_ref[...] = jnp.zeros_like(enter_ref)

    def chain(n):
        @pl.when(z == n)
        def _():
            if n:
                state_b().wait_recv()
                enter_ref[...] = B[1].astype(f32)
            if n < Z - 1:
                through = jnp.exp(state_ref[DV : DV + 1, :]) * enter_ref[...] + state_ref[0:DV, :]
                B[0] = through.astype(bf16)
                state_b().start()

    def enter():
        for n in range(X - 1):
            state = enter_ref[...]
            enter_ref[...] = jnp.where(n < x, fold(A, n, state)[1], state)

    def finish(i):
        at = pl.ds(i * rows, rows)
        state = enter_ref[...].astype(bf16)
        gain = gain_ref[...]
        for h in range(heads):
            ks = slice(h * DK, (h + 1) * DK)
            vs = slice(h * DV, (h + 1) * DV)
            m = mixed_ref[at, vs] + lax.dot_general(
                far_ref[at, ks], state[:, ks], NT, preferred_element_type=f32
            )
            scale = lax.rsqrt(jnp.mean(m * m, axis=-1, keepdims=True) + eps_norm)
            gate = silu(og_ref[at, vs].astype(f32))
            GH[i, tp, :, vs] = (m * scale * gain * gate).astype(bf16)

    order = [z * X + (x + dx) % X for dx in range(X)]
    for j in range(1, Z):
        order += [near(j) * X + (x + dx) % X for dx in range(X)]

    def expert_hidden(pieces, unit):
        for n, h in pieces:
            row_part(order[n], h).wait_recv()
        a = jnp.concatenate([rows_of(order[n], h) for n, h in pieces], axis=0)
        hidden(a, eg_ref, eu_ref, unit)
        unit_send(unit)

    def expert_result(pieces, unit, hold=None):
        unit_wait(unit)
        out = dot(unit_rows(unit), ed_ref[...]).astype(bf16)
        size = part * CORES
        for i, (n, h) in enumerate(pieces):
            RO[n, h] = out[i * size : (i + 1) * size]
        for n, h in pieces:
            if n % X and hold is not None:
                hold.append((n, h))
            elif n:
                send_result(n, h)

    turns = seq // BLOCK
    ahead = 1

    def scan(lo, hi):
        lax.fori_loop(lo, hi, scan_turn, 0, unroll=2)

    for h in range(CH):
        send_own(h)
    own = jnp.concatenate([rows_of(ep, h) for h in range(CH)], axis=0)
    need(sg_ref, su_ref)
    hidden(own, sg_ref, su_ref, shared_unit)
    unit_send(shared_unit)
    need(eg_ref, eu_ref)
    hidden(own, eg_ref, eu_ref, own_unit)
    unit_send(own_unit)
    need(r_ref, b_ref, q_ref, k_ref, v_ref)
    load(late)
    state_ref[...] = jnp.zeros_like(state_ref)
    own_pieces = [(0, h) for h in range(CH)]
    stage_pieces = []

    def states():
        put_state(A, x)
        for dx in range(1, X):
            state_a(dx).start()

    def shared_down():
        need(sd_ref)
        unit_wait(shared_unit)
        acc_ref[...] = dot(unit_rows(shared_unit), sd_ref[...])
        need(ed_ref)
        expert_result(own_pieces, own_unit)

    def forward(unit):
        unit_forward(unit)

    def mixing(what):
        if what == 0:
            combine()
        chain(what)

    scan(0, turns // 2)
    fillers = {
        0: lambda: scan(turns // 2, 3 * turns // 4),
        1: lambda: (scan(3 * turns // 4, turns), states()),
    }
    held = []
    for n in range(stages):
        j, h = n // CH + 1, n % CH
        relay_line(j, h)
        for dx in range(1, X):
            relay_side(j - 1, h, dx)
        if n > stages - Z:
            mixing(n - (stages - Z) - 1)
        stage_pieces.append([((j - 1) * X + dx, h) for dx in range(1, X)] + [(j * X, h)])
        fillers.get(n, lambda: None)()
        if n >= 3:
            expert_result(stage_pieces[n - 3], stage_units[n - 3], held)
        if n == 1:
            forward(shared_unit)
            forward(own_unit)
        if n == 2:
            shared_down()
        expert_hidden(stage_pieces[n], stage_units[n])
        if n >= 2:
            forward(stage_units[n - 2])
    mixing(Z - 1)
    need(og_ref, gain_ref)
    enter()
    for i in range(chunks):
        finish(i)
        if i < ahead:
            unit_send(head_units[i])
    forward(stage_units[-2])
    for n in (stages - 3, stages - 2):
        expert_result(stage_pieces[n], stage_units[n], held)
    last_pieces = [((Z - 1) * X + dx, h) for dx in range(1, X) for h in range(CH)]
    for h in range(CH):
        for dx in range(1, X):
            relay_side(Z - 1, h, dx)
    for piece in held:
        send_result(*piece)
    expert_hidden(last_pieces, last_unit)
    for unit in head_units[ahead:]:
        unit_send(unit)
    forward(stage_units[-1])
    expert_result(stage_pieces[-1], stage_units[-1])
    need(wo_ref)
    need(idx_ref, w_ref)

    index, given = idx_ref[...], w_ref[...]
    by_expert = [jnp.sum(jnp.where(index == e, given, 0.0), axis=0, keepdims=True) for e in range(E)]
    by_expert = jnp.transpose(jnp.concatenate(by_expert, axis=0), (1, 0))
    lane = lax.broadcasted_iota(jnp.int32, by_expert.shape, 1)

    def weight(e):
        return jnp.sum(jnp.where(lane == e, by_expert, 0.0), axis=1, keepdims=True)

    def mixer_out(i):
        at = pl.ds(i * rows, rows)
        return pltpu.make_async_copy(mixer_ref.at[at], mixer_hbm.at[at], out_sem.at[i])

    def mixer(i):
        unit_wait(head_units[i])
        at = pl.ds(i * rows, rows)
        mixer_ref[at, :] = dot(unit_rows(head_units[i]), wo_ref[...]).astype(bf16)
        mixer_out(i).start()

    def add(e, got):
        full = jnp.concatenate([got(h) for h in range(CH)], axis=0)
        acc_ref[...] += full.astype(f32) * weight(e)

    def collect(ns):
        for n in ns:
            e = order[n]
            for h in range(CH):
                remote(RO.at[n, h], RI.at[e, h], res_s.at[0], res_r.at[e, h], e, tp).wait_recv()
            add(e, lambda h: RI[e, h])

    for i in range(ahead):
        forward(head_units[i])
    forward(last_unit)
    for i in range(ahead):
        mixer(i)
    expert_result(last_pieces, last_unit)
    add(ep, lambda h: RO[0, h])
    for i in range(ahead, chunks):
        forward(head_units[i])
        mixer(i)
    collect(range(1, E))
    blend_ref[...] = acc_ref[...].astype(bf16)
    blend_out = pltpu.make_async_copy(blend_ref, blend_hbm, out_sem.at[chunks])
    blend_out.start()

    for h in range(CH):
        pl.when(z < Z - 1)(lambda: row_up(ep, h).wait_send())
        pl.when(z > 0)(lambda: row_down(ep, h, r_down_s.at[h]).wait_send())
        for k in range(1, Z):
            pl.when((z >= k) & (z < Z - 1))(lambda: row_up(ep - k * X, h).wait_send())
            pl.when((z + k < Z) & (z > 0))(lambda: row_down(ep + k * X, h).wait_send())
        for k in range(Z):
            for dx in range(1, X):
                row_x(near(k) * X + x, h, dx).wait_send()
        pl.when(z > 0)(lambda: row_part(ep, h, 0).wait_send())
        pl.when(z < Z - 1)(lambda: row_part(ep, h, 1).wait_send())
        for dx in range(1, X):
            row_part(ep, h, 1 + dx).wait_send()
    for sends in (part_sends, *y_sends, *f_sends, result_sends):
        sends.drain()
    for dx in range(1, X):
        state_a(dx).wait_send()
    pl.when(z < Z - 1)(lambda: state_b().wait_send())
    for i in range(chunks):
        mixer_out(i).wait()
    blend_out.wait()


def local(
    queries,
    sequence_keys,
    stream_content_vectors,
    output_gate_logits,
    retention_preactivation,
    additional_fade_bias,
    attention_group_rescale,
    output_projection,
    expert_batch_tokens,
    expert_norm_gain,
    routed_expert_index,
    routed_expert_weights,
    expert_gate_matrix,
    expert_up_matrix,
    expert_down_matrix,
    shared_gate_matrix,
    shared_up_matrix,
    shared_down_matrix,
):
    experts, lanes = lax.axis_size("ep"), lax.axis_size("tp")
    X = 2 ** (int(math.log2(experts)) // 2)
    Z, Y = experts // X, lanes // CORES
    rows, model_width = expert_batch_tokens.shape
    seq, kw = queries.shape
    vw = stream_content_vectors.shape[1]
    width = shared_gate_matrix.shape[1]
    chunks = seq // rows
    stages = (Z - 1) * CH
    units = 3 + stages + chunks
    args = (
        queries,
        sequence_keys,
        stream_content_vectors,
        output_gate_logits,
        retention_preactivation,
        additional_fade_bias,
        attention_group_rescale.reshape(1, DV),
        output_projection,
        expert_batch_tokens,
        expert_norm_gain.reshape(1, model_width),
        routed_expert_index.T,
        routed_expert_weights.T,
        expert_gate_matrix[0],
        expert_up_matrix[0],
        expert_down_matrix[0],
        shared_gate_matrix,
        shared_up_matrix,
        shared_down_matrix,
    )
    outs = (
        jax.ShapeDtypeStruct((seq, output_projection.shape[1]), bf16),
        jax.ShapeDtypeStruct((rows, shared_down_matrix.shape[1]), bf16),
    )
    dma = lambda *shape: pltpu.SemaphoreType.DMA(shape)
    scratch = [pltpu.VMEM(a.shape, a.dtype) for a in args]
    scratch += [pltpu.VMEM(o.shape, o.dtype) for o in outs]
    scratch += [
        pltpu.VMEM((experts, CH, CORES, rows // (CH * CORES), model_width), bf16),
        pltpu.VMEM((2, lanes, rows, width), bf16),
        pltpu.VMEM((stages, lanes, X * rows // CH, width), bf16),
        pltpu.VMEM((1, lanes, (X - 1) * rows, width), bf16),
        pltpu.VMEM((chunks, lanes, rows, vw), bf16),
        pltpu.VMEM((experts, CH, rows // CH, outs[1].shape[1]), bf16),
        pltpu.VMEM((experts, CH, rows // CH, outs[1].shape[1]), bf16),
        pltpu.VMEM((X, DV + PAD, kw), bf16),
        pltpu.VMEM((2, DV, kw), bf16),
        pltpu.VMEM((seq, vw), f32),
        pltpu.VMEM((seq, kw), bf16),
        pltpu.VMEM((DV + 8, kw), f32),
        pltpu.VMEM((DV, kw), f32),
        pltpu.VMEM((rows, outs[1].shape[1]), f32),
        dma(11),
        dma(chunks + 1),
        dma(1 + X, CH),
        dma(Z, CH),
        dma(CH),
        dma(X - 1, Z, CH),
        dma(experts, CH),
        dma(experts, CH),
        dma(5),
        dma(units),
        dma(Y - 1, 9),
        dma(Y - 1, units),
        dma(Y - 1, 3),
        dma(Y - 1, units),
        dma(14),
        dma(experts, CH),
        dma(X - 1),
        dma(X - 1),
        dma(1),
        dma(1),
    ]
    made = pl.pallas_call(
        functools.partial(body, (Z, X, Y)),
        out_shape=outs,
        in_specs=[pl.BlockSpec(memory_space=pl.ANY)] * len(args),
        out_specs=tuple([pl.BlockSpec(memory_space=pl.ANY)] * len(outs)),
        scratch_shapes=scratch,
        compiler_params=pltpu.CompilerParams(
            collective_id=0, has_side_effects=True, vmem_limit_bytes=66000000
        ),
        cost_estimate=pl.CostEstimate(
            flops=10**10, bytes_accessed=20 * 2**20, transcendentals=10**6
        ),
        name="step",
    )(*args)
    return pl.pallas_call(
        settle,
        out_shape=outs,
        in_specs=[pl.BlockSpec(memory_space=pl.ANY)] * 2,
        out_specs=tuple([pl.BlockSpec(memory_space=pl.ANY)] * 2),
        scratch_shapes=[pltpu.VMEM(o.shape, o.dtype) for o in outs] + [dma(4)],
        cost_estimate=pl.CostEstimate(flops=10**6, bytes_accessed=2**21, transcendentals=0),
        name="settle",
    )(*made)


def settle(mixer_in, blend_in, mixer_out, blend_out, mixer_ref, blend_ref, sem):
    reads = [
        pltpu.make_async_copy(mixer_in, mixer_ref, sem.at[0]),
        pltpu.make_async_copy(blend_in, blend_ref, sem.at[1]),
    ]
    writes = [
        pltpu.make_async_copy(mixer_ref, mixer_out, sem.at[2]),
        pltpu.make_async_copy(blend_ref, blend_out, sem.at[3]),
    ]
    for copy in reads:
        copy.start()
    for read, write in zip(reads, writes):
        read.wait()
        write.start()
    for copy in writes:
        copy.wait()


def solution(mesh):
    in_specs = (
        P("ep", "tp"),
        P("ep", "tp"),
        P("ep", "tp"),
        P("ep", "tp"),
        P("ep", "tp"),
        P("ep", "tp"),
        P(),
        P(None, "tp"),
        P("ep", None),
        P(),
        P("ep", None),
        P("ep", None),
        P("ep", None, "tp"),
        P("ep", None, "tp"),
        P("ep", None, "tp"),
        P(None, "tp"),
        P(None, "tp"),
        P(None, "tp"),
    )
    out_specs = (P("ep", "tp"), P("ep", "tp"))
    return jax.shard_map(local, mesh=mesh, in_specs=in_specs, out_specs=out_specs, check_vma=False)
```

```python
import functools
import math

import jax
import jax.numpy as jnp
from jax import lax
from jax.experimental import pallas as pl
from jax.experimental.pallas import tpu as pltpu
from jax.sharding import PartitionSpec as P

DK = 64
DV = 128
BLOCK = 64
PAD = 16
CORES = 2
CH = 2

eps_norm = 1e-06
switch_softness = 16.0
bf16 = jnp.bfloat16
f32 = jnp.float32
NT = (((1,), (1,)), ((), ()))
TN = (((0,), (0,)), ((), ()))
MESH = pl.DeviceIdType.MESH


def silu(x):
    return x * jax.nn.sigmoid(x)


def dot(a, b):
    return jnp.dot(a, b, preferred_element_type=f32)


def body(sizes, *refs):
    Z, X, Y = sizes
    E, TP = Z * X, Y * CORES
    (
        q_hbm, k_hbm, v_hbm, og_hbm, r_hbm, b_hbm, gain_hbm, wo_hbm, tok_hbm, ng_hbm, idx_hbm, w_hbm,
        eg_hbm, eu_hbm, ed_hbm, sg_hbm, su_hbm, sd_hbm,
        mixer_ref, blend_ref,
        q_ref, k_ref, v_ref, og_ref, r_ref, b_ref, gain_ref, wo_ref, tok_ref, ng_ref, idx_ref, w_ref,
        eg_ref, eu_ref, ed_ref, sg_ref, su_ref, sd_ref,
        R, GS, GE, GL, GH, RO, RI, A, B, mixed_ref, far_ref, state_ref, enter_ref, acc_ref,
        in_sem,
        r_part_s, r_z_s, r_down_s, r_x_s, r_side_s, r_far_r, r_part_r,
        u_part_s, u_part_r, u_y_s, u_y_r, u_f_s, u_f_r,
        res_s, res_r, a_s, a_r, b_s, b_r,
    ) = refs

    ep, tp = lax.axis_index("ep"), lax.axis_index("tp")
    z, x = ep // X, ep % X
    y, c = tp // CORES, tp % CORES
    partner = y * CORES + (1 - c)
    rows = tok_ref.shape[0]
    seq, kw = q_ref.shape
    heads = kw // DK
    chunks = seq // rows
    width = GS.shape[-1]
    part = rows // (CH * CORES)

    def remote(src, dst, ssem, rsem, e, t):
        return pltpu.make_async_remote_copy(
            src_ref=src,
            dst_ref=dst,
            send_sem=ssem,
            recv_sem=rsem,
            device_id={"ep": e, "tp": t},
            device_id_type=MESH,
        )

    early = [
        (tok_hbm, tok_ref), (ng_hbm, ng_ref), (sg_hbm, sg_ref), (su_hbm, su_ref), (eg_hbm, eg_ref), (eu_hbm, eu_ref),
        (r_hbm, r_ref), (b_hbm, b_ref), (q_hbm, q_ref), (k_hbm, k_ref), (v_hbm, v_ref),
    ]
    late = [
        (sd_hbm, sd_ref), (ed_hbm, ed_ref), (og_hbm, og_ref), (gain_hbm, gain_ref), (wo_hbm, wo_ref),
        (idx_hbm, idx_ref), (w_hbm, w_ref),
    ]
    copies = {}

    def load(pairs):
        for n, (src, dst) in enumerate(pairs):
            copies[id(dst)] = pltpu.make_async_copy(src, dst, in_sem.at[n])
            copies[id(dst)].start()

    load(early)

    def need(*dsts):
        for dst in dsts:
            copies[id(dst)].wait()

    class Sends:
        def __init__(self, sems, count):
            self.sems, self.count, self.sent, self.held = sems, count, 0, {}

        def start(self, make):
            n = self.sent % self.count
            if n in self.held:
                self.held[n].wait_send()
            self.held[n] = make(self.sems.at[n])
            self.held[n].start()
            self.sent += 1

        def drain(self):
            for copy in self.held.values():
                copy.wait_send()

    barrier = pltpu.get_barrier_semaphore()

    def greet(e, t):
        pl.semaphore_signal(barrier, inc=1, device_id={"ep": e, "tp": t}, device_id_type=MESH)

    greet(ep, partner)
    for dy in range(1, Y):
        greet(ep, (y + dy) % Y * CORES + c)
    for dx in range(1, X):
        greet(z * X + (x + dx) % X, tp)
    pl.when(z < Z - 1)(lambda: greet(ep + X, tp))
    pl.when(z > 0)(lambda: greet(ep - X, tp))

    need(tok_ref, ng_ref)
    flat = tok_ref[...].astype(f32)
    normed = (
        flat * lax.rsqrt(jnp.mean(flat * flat, axis=-1, keepdims=True) + eps_norm) * ng_ref[...]
    ).astype(bf16)
    for n in range(CH * CORES):
        R[ep, n // CORES, n % CORES] = normed[n * part : (n + 1) * part]

    lines = jnp.where(z < Z - 1, 1, 0) + jnp.where(z > 0, 1, 0)
    pl.semaphore_wait(barrier, 1 + (Y - 1) + (X - 1) + lines)

    def row_part(b, h, kind=0):
        return remote(R.at[b, h, c], R.at[b, h, c], r_part_s.at[kind, h], r_part_r.at[b, h], ep, partner)

    def row_up(b, h):
        return remote(R.at[b, h, c], R.at[b, h, c], r_z_s.at[b // X, h], r_far_r.at[b, h], ep + X, tp)

    def row_down(b, h, sem=None):
        sem = r_z_s.at[b // X, h] if sem is None else sem
        return remote(R.at[b, h, c], R.at[b, h, c], sem, r_far_r.at[b, h], ep - X, tp)

    def row_x(b, h, dx):
        there = z * X + (x + dx) % X
        return remote(R.at[b, h, c], R.at[b, h, c], r_x_s.at[dx - 1, b // X, h], r_far_r.at[b, h], there, tp)

    def near(j):
        up = jnp.where(j <= Z - 1 - z, z + j, Z - 1 - j)
        down = jnp.where(j <= z, z - j, j)
        return jnp.where(2 * z < Z, up, down)

    def send_own(h):
        pl.when(z < Z - 1)(lambda: row_up(ep, h).start())
        pl.when(z > 0)(lambda: row_down(ep, h, r_down_s.at[h]).start())
        for dx in range(1, X):
            row_x(ep, h, dx).start()

    def arrive(b, h):
        remote(R.at[b, h, c], R.at[b, h, c], r_part_s.at[0, h], r_far_r.at[b, h], ep, partner).wait_recv()

    def hand_over(b, h, kind, again):
        copy = row_part(b, h, kind)
        if again:
            copy.wait_send()
        copy.start()

    def relay_line(k, h):
        @pl.when(z >= k)
        def _():
            b = ep - k * X
            arrive(b, h)
            pl.when(z < Z - 1)(lambda: row_up(b, h).start())
            hand_over(b, h, 0, k > 1)

        @pl.when(z + k < Z)
        def _():
            b = ep + k * X
            arrive(b, h)
            pl.when(z > 0)(lambda: row_down(b, h).start())
            hand_over(b, h, 1, k > 1)

        @pl.when(inner(near(k)))
        def _():
            for dx in range(1, X):
                row_x(near(k) * X + x, h, dx).start()

    def inner(zj):
        return (zj > 0) & (zj < Z - 1)

    def side(j, dx):
        return near(j) * X + (x + dx) % X

    def top(dx):
        return (Z - 1) * X + (x + dx) % X

    def bottom(dx):
        return (x + dx) % X

    def side_row(b, h, up, dx):
        there = ep + X if up else ep - X
        sem = r_side_s.at[dx - 1, int(up), h]
        return remote(R.at[b, h, c], R.at[b, h, c], sem, r_far_r.at[b, h], there, tp)

    def relay_side(j, h, dx):
        kind = 2 + (dx - 1) * (Z + 2)

        def here(b, n):
            arrive(b, h)
            row_part(b, h, kind + n).start()

        if j == 0:
            here(side(0, dx), 0)
            pl.when(z == 0)(lambda: side_row(bottom(dx), h, True, dx).start())
            pl.when(z == Z - 1)(lambda: side_row(top(dx), h, False, dx).start())
            return

        pl.when(inner(near(j)))(lambda: here(side(j, dx), j))

        @pl.when(z == Z - 1 - j)
        def _():
            here(top(dx), Z)
            pl.when(z > 0)(lambda: side_row(top(dx), h, False, dx).start())

        @pl.when(z == j)
        def _():
            here(bottom(dx), Z + 1)
            pl.when(z < Z - 1)(lambda: side_row(bottom(dx), h, True, dx).start())

    def rows_of(b, h):
        return jnp.concatenate([R[b, h, n] for n in range(CORES)], axis=0)

    part_sends = Sends(u_part_s, u_part_s.shape[0])
    y_sends = [Sends(u_y_s.at[n], u_y_s.shape[1]) for n in range(Y - 1)]
    f_sends = [Sends(u_f_s.at[n], u_f_s.shape[1]) for n in range(Y - 1)]
    result_sends = Sends(res_s, res_s.shape[0])

    def unit_part(unit, sem=None):
        G, n, u = unit
        sem = u_part_s.at[0] if sem is None else sem
        return remote(G.at[n, tp], G.at[n, tp], sem, u_part_r.at[u], ep, partner)

    def unit_y(unit, dy, sem=None):
        G, n, u = unit
        t = (y + dy) % Y * CORES + c
        sem = u_y_s.at[dy - 1, 0] if sem is None else sem
        return remote(G.at[n, tp], G.at[n, tp], sem, u_y_r.at[dy - 1, u], ep, t)

    def unit_f(unit, dy, sem=None):
        G, n, u = unit
        t = (y - dy + Y) % Y * CORES + c
        sem = u_f_s.at[dy - 1, 0] if sem is None else sem
        return remote(G.at[n, t], G.at[n, t], sem, u_f_r.at[dy - 1, u], ep, partner)

    def unit_send(unit):
        for dy in range(1, Y):
            y_sends[dy - 1].start(lambda sem: unit_y(unit, dy, sem))
        part_sends.start(lambda sem: unit_part(unit, sem))

    def unit_forward(unit):
        for dy in range(1, Y):
            unit_y(unit, dy).wait_recv()
            f_sends[dy - 1].start(lambda sem: unit_f(unit, dy, sem))

    def unit_wait(unit):
        unit_part(unit).wait_recv()
        for dy in range(1, Y):
            unit_f(unit, dy).wait_recv()

    def unit_rows(unit):
        return jnp.concatenate([unit[0][unit[1], t] for t in range(TP)], axis=1)

    shared_unit, own_unit = (GS, 0, 0), (GS, 1, 1)
    stages = (Z - 1) * CH
    stage_units = [(GE, n, 2 + n) for n in range(stages)]
    last_unit = (GL, 0, 2 + stages)
    head_units = [(GH, n, 3 + stages + n) for n in range(chunks)]

    tile = min(256, width)

    def hidden(a, gate_w, up_w, unit):
        def turn(n, carry):
            at = pl.ds(pl.multiple_of(n * tile, tile), tile)
            h = silu(dot(a, gate_w[:, at])) * dot(a, up_w[:, at])
            unit[0][unit[1], tp, :, at] = h.astype(bf16)
            return carry

        lax.fori_loop(0, width // tile, turn, 0)

    def send_result(n, h):
        result_sends.start(
            lambda sem: remote(RO.at[n, h], RI.at[ep, h], sem, res_r.at[ep, h], order[n], tp)
        )

    row = lax.broadcasted_iota(jnp.int32, (BLOCK, BLOCK), 0)
    col = lax.broadcasted_iota(jnp.int32, (BLOCK, BLOCK), 1)
    causal = row >= col
    tril = causal.astype(f32)

    def scan_turn(n, _):
        at = pl.ds(pl.multiple_of(n * BLOCK, BLOCK), BLOCK)
        r = r_ref[at, :].astype(f32)
        log_sig = jnp.minimum(r, 0.0) - jnp.log1p(jnp.exp(-jnp.abs(r)))
        rate = log_sig / switch_softness + b_ref[at, :]
        inner = jnp.dot(tril, rate, precision=lax.Precision.HIGHEST, preferred_element_type=f32)
        last = inner[BLOCK - 1 : BLOCK, :]
        q = q_ref[at, :].astype(f32) * DK**-0.5
        k = k_ref[at, :].astype(f32)
        q_in = q * jnp.exp(inner)
        q_b = q_in.astype(bf16)
        k_b = (k * jnp.exp(-inner)).astype(bf16)
        k_out = (k * jnp.exp(last - inner)).astype(bf16)
        prior = state_ref[DV : DV + 1, :]
        far_ref[at, :] = (q * jnp.exp(inner + prior)).astype(bf16)
        entering = state_ref[0:DV, :]
        entering_b = entering.astype(bf16)
        updates = []
        for h in range(heads):
            ks = slice(h * DK, (h + 1) * DK)
            vs = slice(h * DV, (h + 1) * DV)
            v = v_ref[at, vs]
            scores = lax.dot_general(q_b[:, ks], k_b[:, ks], NT, preferred_element_type=f32)
            scores = jnp.where(causal, scores, 0.0).astype(bf16)
            out = jnp.dot(scores, v, preferred_element_type=f32)
            out += lax.dot_general(q_b[:, ks], entering_b[:, ks], NT, preferred_element_type=f32)
            mixed_ref[at, vs] = out
            updates.append(lax.dot_general(v, k_out[:, ks], TN, preferred_element_type=f32))
        state_ref[0:DV, :] = entering * jnp.exp(last) + jnp.concatenate(updates, axis=1)
        state_ref[DV : DV + 1, :] = prior + last
        return 0

    def put_state(dst, n):
        fade = state_ref[DV : DV + 8, :]
        high = fade.astype(bf16)
        low = (fade - high.astype(f32)).astype(bf16)
        dst[n, 0:DV, :] = state_ref[0:DV, :].astype(bf16)
        dst[n, DV : DV + PAD, :] = jnp.concatenate([high, low], axis=0)

    def state_a(dx):
        return remote(A.at[x], A.at[x], a_s.at[dx - 1], a_r.at[dx - 1], z * X + (x + dx) % X, tp)

    def state_b():
        return remote(B.at[0], B.at[1], b_s.at[0], b_r.at[0], (ep + X) % E, tp)

    def fold(src, n, state):
        fade = src[n, DV : DV + PAD, :].astype(f32)
        fade = fade[0:8] + fade[8:16]
        return fade, jnp.exp(fade[0:1]) * state + src[n, 0:DV, :].astype(f32)

    def combine():
        for dx in range(1, X):
            state_a(dx).wait_recv()
        state = jnp.zeros((DV, kw), f32)
        total = jnp.zeros((8, kw), f32)
        for n in range(X):
            fade, state = fold(A, n, state)
            total += fade
        state_ref[0:DV, :] = state
        state_ref[DV : DV + 8, :] = total
        enter_ref[...] = jnp.zeros_like(enter_ref)

    def chain(n):
        @pl.when(z == n)
        def _():
            if n:
                state_b().wait_recv()
                enter_ref[...] = B[1].astype(f32)
            if n < Z - 1:
                through = jnp.exp(state_ref[DV : DV + 1, :]) * enter_ref[...] + state_ref[0:DV, :]
                B[0] = through.astype(bf16)
                state_b().start()

    def enter():
        for n in range(X - 1):
            state = enter_ref[...]
            enter_ref[...] = jnp.where(n < x, fold(A, n, state)[1], state)

    def finish(i):
        at = pl.ds(i * rows, rows)
        state = enter_ref[...].astype(bf16)
        gain = gain_ref[...]
        for h in range(heads):
            ks = slice(h * DK, (h + 1) * DK)
            vs = slice(h * DV, (h + 1) * DV)
            m = mixed_ref[at, vs] + lax.dot_general(
                far_ref[at, ks], state[:, ks], NT, preferred_element_type=f32
            )
            scale = lax.rsqrt(jnp.mean(m * m, axis=-1, keepdims=True) + eps_norm)
            gate = silu(og_ref[at, vs].astype(f32))
            GH[i, tp, :, vs] = (m * scale * gain * gate).astype(bf16)

    order = [z * X + (x + dx) % X for dx in range(X)]
    for j in range(1, Z):
        order += [near(j) * X + (x + dx) % X for dx in range(X)]

    def expert_hidden(pieces, unit):
        for n, h in pieces:
            row_part(order[n], h).wait_recv()
        a = jnp.concatenate([rows_of(order[n], h) for n, h in pieces], axis=0)
        hidden(a, eg_ref, eu_ref, unit)
        unit_send(unit)

    def expert_result(pieces, unit, hold=None):
        unit_wait(unit)
        out = dot(unit_rows(unit), ed_ref[...]).astype(bf16)
        size = part * CORES
        for i, (n, h) in enumerate(pieces):
            RO[n, h] = out[i * size : (i + 1) * size]
        for n, h in pieces:
            if n % X and hold is not None:
                hold.append((n, h))
            elif n:
                send_result(n, h)

    turns = seq // BLOCK

    def scan(lo, hi):
        lax.fori_loop(lo, hi, scan_turn, 0, unroll=2)

    for h in range(CH):
        send_own(h)
    own = jnp.concatenate([rows_of(ep, h) for h in range(CH)], axis=0)
    need(sg_ref, su_ref)
    hidden(own, sg_ref, su_ref, shared_unit)
    unit_send(shared_unit)
    need(eg_ref, eu_ref)
    hidden(own, eg_ref, eu_ref, own_unit)
    unit_send(own_unit)
    need(r_ref, b_ref, q_ref, k_ref, v_ref)
    load(late)
    state_ref[...] = jnp.zeros_like(state_ref)
    own_pieces = [(0, h) for h in range(CH)]
    stage_pieces = []

    def states():
        put_state(A, x)
        for dx in range(1, X):
            state_a(dx).start()

    def shared_down():
        need(sd_ref)
        unit_wait(shared_unit)
        acc_ref[...] = dot(unit_rows(shared_unit), sd_ref[...])
        need(ed_ref)
        expert_result(own_pieces, own_unit)

    def forward(unit):
        unit_forward(unit)

    def mixing(what):
        if what == 0:
            combine()
        chain(what)

    scan(0, turns // 2)
    fillers = {
        0: lambda: scan(turns // 2, 3 * turns // 4),
        1: lambda: (scan(3 * turns // 4, turns), states()),
    }
    held = []
    for n in range(stages):
        j, h = n // CH + 1, n % CH
        relay_line(j, h)
        for dx in range(1, X):
            relay_side(j - 1, h, dx)
        stage_pieces.append([((j - 1) * X + dx, h) for dx in range(1, X)] + [(j * X, h)])
        fillers.get(n, lambda: None)()
        if n == stages - 1:
            for piece in held:
                send_result(*piece)
            held = None
        if n >= 3:
            expert_result(stage_pieces[n - 3], stage_units[n - 3], held)
        if n == 1:
            forward(shared_unit)
            forward(own_unit)
        if n == 2:
            shared_down()
        expert_hidden(stage_pieces[n], stage_units[n])
        if n > stages - Z:
            mixing(n - (stages - Z) - 1)
        if n >= 2:
            forward(stage_units[n - 2])
    last_pieces = [((Z - 1) * X + dx, h) for dx in range(1, X) for h in range(CH)]
    for h in range(CH):
        for dx in range(1, X):
            relay_side(Z - 1, h, dx)
    for piece in held or ():
        send_result(*piece)
    expert_result(stage_pieces[stages - 3], stage_units[stages - 3])
    expert_hidden(last_pieces, last_unit)
    forward(stage_units[-2])
    mixing(Z - 1)
    need(og_ref, gain_ref)
    enter()
    for i in range(chunks // 2):
        finish(i)
        unit_send(head_units[i])
    expert_result(stage_pieces[-2], stage_units[-2])
    for i in range(chunks // 2, chunks):
        finish(i)
        unit_send(head_units[i])
    forward(stage_units[-1])
    expert_result(stage_pieces[-1], stage_units[-1])
    need(wo_ref)
    need(idx_ref, w_ref)

    index, given = idx_ref[...], w_ref[...]
    by_expert = [jnp.sum(jnp.where(index == e, given, 0.0), axis=0, keepdims=True) for e in range(E)]
    by_expert = jnp.transpose(jnp.concatenate(by_expert, axis=0), (1, 0))
    lane = lax.broadcasted_iota(jnp.int32, by_expert.shape, 1)

    def weight(e):
        return jnp.sum(jnp.where(lane == e, by_expert, 0.0), axis=1, keepdims=True)

    def mixer(i):
        unit_wait(head_units[i])
        at = pl.ds(i * rows, rows)
        mixer_ref[at, :] = dot(unit_rows(head_units[i]), wo_ref[...]).astype(bf16)

    def add(e, got):
        full = jnp.concatenate([got(h) for h in range(CH)], axis=0)
        acc_ref[...] += full.astype(f32) * weight(e)

    def collect(ns):
        for n in ns:
            e = order[n]
            for h in range(CH):
                remote(RO.at[n, h], RI.at[e, h], res_s.at[0], res_r.at[e, h], e, tp).wait_recv()
            add(e, lambda h: RI[e, h])

    forward(last_unit)
    expert_result(last_pieces, last_unit)
    add(ep, lambda h: RO[0, h])
    for i in range(chunks):
        forward(head_units[i])
        mixer(i)
    collect(range(1, E))
    blend_ref[...] = acc_ref[...].astype(bf16)

    for h in range(CH):
        pl.when(z < Z - 1)(lambda: row_up(ep, h).wait_send())
        pl.when(z > 0)(lambda: row_down(ep, h, r_down_s.at[h]).wait_send())
        for k in range(1, Z):
            pl.when((z >= k) & (z < Z - 1))(lambda: row_up(ep - k * X, h).wait_send())
            pl.when((z + k < Z) & (z > 0))(lambda: row_down(ep + k * X, h).wait_send())
        for dx in range(1, X):
            kind = 2 + (dx - 1) * (Z + 2)
            row_x(ep, h, dx).wait_send()
            row_part(ep, h, kind).wait_send()
            for k in range(1, Z):
                pl.when(inner(near(k)))(lambda: row_x(near(k) * X + x, h, dx).wait_send())
                pl.when(inner(near(k)))(lambda: row_part(ep, h, kind + k).wait_send())
            pl.when(z < Z - 1)(lambda: row_part(ep, h, kind + Z).wait_send())
            pl.when(z > 0)(lambda: row_part(ep, h, kind + Z + 1).wait_send())
            pl.when(z < Z - 1)(lambda: side_row(ep, h, True, dx).wait_send())
            pl.when(z > 0)(lambda: side_row(ep, h, False, dx).wait_send())
        pl.when(z > 0)(lambda: row_part(ep, h, 0).wait_send())
        pl.when(z < Z - 1)(lambda: row_part(ep, h, 1).wait_send())
    for sends in (part_sends, *y_sends, *f_sends, result_sends):
        sends.drain()
    for dx in range(1, X):
        state_a(dx).wait_send()
    pl.when(z < Z - 1)(lambda: state_b().wait_send())


def local(
    queries,
    sequence_keys,
    stream_content_vectors,
    output_gate_logits,
    retention_preactivation,
    additional_fade_bias,
    attention_group_rescale,
    output_projection,
    expert_batch_tokens,
    expert_norm_gain,
    routed_expert_index,
    routed_expert_weights,
    expert_gate_matrix,
    expert_up_matrix,
    expert_down_matrix,
    shared_gate_matrix,
    shared_up_matrix,
    shared_down_matrix,
):
    experts, lanes = lax.axis_size("ep"), lax.axis_size("tp")
    X = 2 ** (int(math.log2(experts)) // 2)
    Z, Y = experts // X, lanes // CORES
    rows, model_width = expert_batch_tokens.shape
    seq, kw = queries.shape
    vw = stream_content_vectors.shape[1]
    width = shared_gate_matrix.shape[1]
    chunks = seq // rows
    stages = (Z - 1) * CH
    units = 3 + stages + chunks
    args = (
        queries,
        sequence_keys,
        stream_content_vectors,
        output_gate_logits,
        retention_preactivation,
        additional_fade_bias,
        attention_group_rescale.reshape(1, DV),
        output_projection,
        expert_batch_tokens,
        expert_norm_gain.reshape(1, model_width),
        routed_expert_index.T,
        routed_expert_weights.T,
        expert_gate_matrix[0],
        expert_up_matrix[0],
        expert_down_matrix[0],
        shared_gate_matrix,
        shared_up_matrix,
        shared_down_matrix,
    )
    outs = (
        jax.ShapeDtypeStruct((seq, output_projection.shape[1]), bf16),
        jax.ShapeDtypeStruct((rows, shared_down_matrix.shape[1]), bf16),
    )
    dma = lambda *shape: pltpu.SemaphoreType.DMA(shape)
    scratch = [pltpu.VMEM(a.shape, a.dtype) for a in args]
    scratch += [
        pltpu.VMEM((experts, CH, CORES, rows // (CH * CORES), model_width), bf16),
        pltpu.VMEM((2, lanes, rows, width), bf16),
        pltpu.VMEM((stages, lanes, X * rows // CH, width), bf16),
        pltpu.VMEM((1, lanes, (X - 1) * rows, width), bf16),
        pltpu.VMEM((chunks, lanes, rows, vw), bf16),
        pltpu.VMEM((experts, CH, rows // CH, outs[1].shape[1]), bf16),
        pltpu.VMEM((experts, CH, rows // CH, outs[1].shape[1]), bf16),
        pltpu.VMEM((X, DV + PAD, kw), bf16),
        pltpu.VMEM((2, DV, kw), bf16),
        pltpu.VMEM((seq, vw), f32),
        pltpu.VMEM((seq, kw), bf16),
        pltpu.VMEM((DV + 8, kw), f32),
        pltpu.VMEM((DV, kw), f32),
        pltpu.VMEM((rows, outs[1].shape[1]), f32),
        dma(11),
        dma(2 + (X - 1) * (Z + 2), CH),
        dma(Z, CH),
        dma(CH),
        dma(X - 1, Z, CH),
        dma(X - 1, 2, CH),
        dma(experts, CH),
        dma(experts, CH),
        dma(5),
        dma(units),
        dma(Y - 1, 9),
        dma(Y - 1, units),
        dma(Y - 1, 3),
        dma(Y - 1, units),
        dma(14),
        dma(experts, CH),
        dma(X - 1),
        dma(X - 1),
        dma(1),
        dma(1),
    ]
    made = pl.pallas_call(
        functools.partial(body, (Z, X, Y)),
        out_shape=tuple(pltpu.VMEM(o.shape, o.dtype) for o in outs),
        in_specs=[pl.BlockSpec(memory_space=pl.ANY)] * len(args),
        out_specs=tuple([pl.BlockSpec(memory_space=pltpu.VMEM)] * len(outs)),
        scratch_shapes=scratch,
        compiler_params=pltpu.CompilerParams(
            collective_id=0, has_side_effects=True, vmem_limit_bytes=66000000
        ),
        cost_estimate=pl.CostEstimate(
            flops=10**10, bytes_accessed=20 * 2**20, transcendentals=10**6
        ),
        name="step",
    )(*args)
    return pl.pallas_call(
        settle,
        out_shape=outs,
        in_specs=[pl.BlockSpec(memory_space=pltpu.VMEM)] * 2,
        out_specs=tuple([pl.BlockSpec(memory_space=pl.ANY)] * 2),
        scratch_shapes=[dma(2)],
        cost_estimate=pl.CostEstimate(flops=10**6, bytes_accessed=2**21, transcendentals=0),
        name="settle",
    )(*[pltpu.with_memory_space_constraint(m, pltpu.VMEM) for m in made])


def settle(mixer_ref, blend_ref, mixer_out, blend_out, sem):
    writes = [
        pltpu.make_async_copy(mixer_ref, mixer_out, sem.at[0]),
        pltpu.make_async_copy(blend_ref, blend_out, sem.at[1]),
    ]
    for copy in writes:
        copy.start()
    for copy in writes:
        copy.wait()


def solution(mesh):
    in_specs = (
        P("ep", "tp"),
        P("ep", "tp"),
        P("ep", "tp"),
        P("ep", "tp"),
        P("ep", "tp"),
        P("ep", "tp"),
        P(),
        P(None, "tp"),
        P("ep", None),
        P(),
        P("ep", None),
        P("ep", None),
        P("ep", None, "tp"),
        P("ep", None, "tp"),
        P("ep", None, "tp"),
        P(None, "tp"),
        P(None, "tp"),
        P(None, "tp"),
    )
    out_specs = (P("ep", "tp"), P("ep", "tp"))
    return jax.shard_map(local, mesh=mesh, in_specs=in_specs, out_specs=out_specs, check_vma=False)
```

```python
import functools
import math

import jax
import jax.numpy as jnp
from jax import lax
from jax.experimental import pallas as pl
from jax.experimental.pallas import tpu as pltpu
from jax.sharding import PartitionSpec as P

DK = 64
DV = 128
BLOCK = 64
PAD = 16
CORES = 2
CH = 2

eps_norm = 1e-06
switch_softness = 16.0
bf16 = jnp.bfloat16
f32 = jnp.float32
NT = (((1,), (1,)), ((), ()))
TN = (((0,), (0,)), ((), ()))
MESH = pl.DeviceIdType.MESH


def silu(x):
    return x * jax.nn.sigmoid(x)


def dot(a, b):
    return jnp.dot(a, b, preferred_element_type=f32)


def body(sizes, *refs):
    Z, X, Y = sizes
    E = Z * X
    (
        q_hbm, k_hbm, v_hbm, og_hbm, r_hbm, b_hbm, gain_hbm, wo_hbm, tok_hbm, ng_hbm, idx_hbm, w_hbm,
        eg_hbm, eu_hbm, ed_hbm, sg_hbm, su_hbm, sd_hbm,
        mixer_ref, blend_ref,
        q_ref, k_ref, v_ref, og_ref, r_ref, b_ref, gain_ref, wo_ref, tok_ref, ng_ref, idx_ref, w_ref,
        eg_ref, eu_ref, ed_ref, sg_ref, su_ref, sd_ref,
        R, GS, GE, GL, GH, RO, RI, A, B, mixed_ref, far_ref, state_ref, enter_ref, acc_ref,
        in_sem,
        r_part_s, r_z_s, r_down_s, r_x_s, r_side_s, r_far_r, r_part_r,
        u_part_s, u_part_r, u_y_s, u_y_r, u_f_s, u_f_r,
        res_s, res_r, a_s, a_r, b_s, b_r,
    ) = refs

    ep, tp = lax.axis_index("ep"), lax.axis_index("tp")
    z, x = ep // X, ep % X
    y, c = tp // CORES, tp % CORES
    partner = y * CORES + (1 - c)
    rows = tok_ref.shape[0]
    seq, kw = q_ref.shape
    heads = kw // DK
    chunks = seq // rows
    tiles, tile = GS.shape[2], GS.shape[-1]
    width = tiles * tile
    part = rows // (CH * CORES)

    def remote(src, dst, ssem, rsem, e, t):
        return pltpu.make_async_remote_copy(
            src_ref=src,
            dst_ref=dst,
            send_sem=ssem,
            recv_sem=rsem,
            device_id={"ep": e, "tp": t},
            device_id_type=MESH,
        )

    early = [
        (tok_hbm, tok_ref), (ng_hbm, ng_ref), (sg_hbm, sg_ref), (su_hbm, su_ref), (eg_hbm, eg_ref), (eu_hbm, eu_ref),
        (r_hbm, r_ref), (b_hbm, b_ref), (q_hbm, q_ref), (k_hbm, k_ref), (v_hbm, v_ref),
    ]
    late = [
        (sd_hbm, sd_ref), (ed_hbm, ed_ref), (og_hbm, og_ref), (gain_hbm, gain_ref), (wo_hbm, wo_ref),
        (idx_hbm, idx_ref), (w_hbm, w_ref),
    ]
    copies = {}

    def load(pairs):
        for n, (src, dst) in enumerate(pairs):
            copies[id(dst)] = pltpu.make_async_copy(src, dst, in_sem.at[n])
            copies[id(dst)].start()

    load(early)

    def need(*dsts):
        for dst in dsts:
            copies[id(dst)].wait()

    class Sends:
        def __init__(self, sems, count):
            self.sems, self.count, self.sent, self.held = sems, count, 0, {}

        def start(self, make):
            n = self.sent % self.count
            if n in self.held:
                self.held[n].wait_send()
            self.held[n] = make(self.sems.at[n])
            self.held[n].start()
            self.sent += 1

        def drain(self):
            for copy in self.held.values():
                copy.wait_send()

    barrier = pltpu.get_barrier_semaphore()

    def greet(e, t):
        pl.semaphore_signal(barrier, inc=1, device_id={"ep": e, "tp": t}, device_id_type=MESH)

    greet(ep, partner)
    for dy in range(1, Y):
        greet(ep, (y + dy) % Y * CORES + c)
    for dx in range(1, X):
        greet(z * X + (x + dx) % X, tp)
    pl.when(z < Z - 1)(lambda: greet(ep + X, tp))
    pl.when(z > 0)(lambda: greet(ep - X, tp))

    need(tok_ref, ng_ref)
    flat = tok_ref[...].astype(f32)
    normed = (
        flat * lax.rsqrt(jnp.mean(flat * flat, axis=-1, keepdims=True) + eps_norm) * ng_ref[...]
    ).astype(bf16)
    for n in range(CH * CORES):
        R[ep, n // CORES, n % CORES] = normed[n * part : (n + 1) * part]

    lines = jnp.where(z < Z - 1, 1, 0) + jnp.where(z > 0, 1, 0)
    pl.semaphore_wait(barrier, 1 + (Y - 1) + (X - 1) + lines)

    def row_part(b, h, kind=0):
        return remote(R.at[b, h, c], R.at[b, h, c], r_part_s.at[kind, h], r_part_r.at[b, h], ep, partner)

    def row_up(b, h):
        return remote(R.at[b, h, c], R.at[b, h, c], r_z_s.at[b // X, h], r_far_r.at[b, h], ep + X, tp)

    def row_down(b, h, sem=None):
        sem = r_z_s.at[b // X, h] if sem is None else sem
        return remote(R.at[b, h, c], R.at[b, h, c], sem, r_far_r.at[b, h], ep - X, tp)

    def row_x(b, h, dx):
        there = z * X + (x + dx) % X
        return remote(R.at[b, h, c], R.at[b, h, c], r_x_s.at[dx - 1, b // X, h], r_far_r.at[b, h], there, tp)

    def near(j):
        up = jnp.where(j <= Z - 1 - z, z + j, Z - 1 - j)
        down = jnp.where(j <= z, z - j, j)
        return jnp.where(2 * z < Z, up, down)

    def send_own(h):
        pl.when(z < Z - 1)(lambda: row_up(ep, h).start())
        pl.when(z > 0)(lambda: row_down(ep, h, r_down_s.at[h]).start())
        for dx in range(1, X):
            row_x(ep, h, dx).start()

    def arrive(b, h):
        remote(R.at[b, h, c], R.at[b, h, c], r_part_s.at[0, h], r_far_r.at[b, h], ep, partner).wait_recv()

    def hand_over(b, h, kind, again):
        copy = row_part(b, h, kind)
        if again:
            copy.wait_send()
        copy.start()

    def relay_line(k, h):
        @pl.when(z >= k)
        def _():
            b = ep - k * X
            arrive(b, h)
            pl.when(z < Z - 1)(lambda: row_up(b, h).start())
            hand_over(b, h, 0, k > 1)

        @pl.when(z + k < Z)
        def _():
            b = ep + k * X
            arrive(b, h)
            pl.when(z > 0)(lambda: row_down(b, h).start())
            hand_over(b, h, 1, k > 1)

        @pl.when(by_x(near(k), h))
        def _():
            for dx in range(1, X):
                row_x(near(k) * X + x, h, dx).start()

    def by_x(zj, h):
        use = (zj > 0) & (zj < Z - 1)
        if h == CH - 1:
            use |= (zj + z == Z - 1) & ((z == 0) | (z == Z - 1))
        return use

    def spare(h):
        return 1 if h == CH - 1 else 0

    def side(j, dx):
        return near(j) * X + (x + dx) % X

    def top(dx):
        return (Z - 1) * X + (x + dx) % X

    def bottom(dx):
        return (x + dx) % X

    def side_row(b, h, up, dx):
        there = ep + X if up else ep - X
        sem = r_side_s.at[dx - 1, int(up), h]
        return remote(R.at[b, h, c], R.at[b, h, c], sem, r_far_r.at[b, h], there, tp)

    def relay_side(j, h, dx):
        kind = 2 + (dx - 1) * (Z + 2)

        def here(b, n):
            arrive(b, h)
            row_part(b, h, kind + n).start()

        if j == 0:
            here(side(0, dx), 0)
            pl.when(z == 0)(lambda: side_row(bottom(dx), h, True, dx).start())
            pl.when(z == Z - 1)(lambda: side_row(top(dx), h, False, dx).start())
            return

        pl.when((near(j) > 0) & (near(j) < Z - 1))(lambda: here(side(j, dx), j))

        @pl.when(z == Z - 1 - j)
        def _():
            here(top(dx), Z)
            pl.when(z > spare(h))(lambda: side_row(top(dx), h, False, dx).start())

        @pl.when(z == j)
        def _():
            here(bottom(dx), Z + 1)
            pl.when(z < Z - 1 - spare(h))(lambda: side_row(bottom(dx), h, True, dx).start())

    def rows_of(b, h):
        return jnp.concatenate([R[b, h, n] for n in range(CORES)], axis=0)

    part_sends = Sends(u_part_s, u_part_s.shape[0])
    y_sends = [Sends(u_y_s.at[n], u_y_s.shape[1]) for n in range(Y - 1)]
    f_sends = [Sends(u_f_s.at[n], u_f_s.shape[1]) for n in range(Y - 1)]
    result_sends = Sends(res_s, res_s.shape[0])

    def unit_part(unit, sem=None):
        G, n, u = unit
        sem = u_part_s.at[0] if sem is None else sem
        return remote(G.at[n, tp], G.at[n, tp], sem, u_part_r.at[u], ep, partner)

    def unit_y(unit, dy, m, sem=None):
        G, n, u = unit
        t = (y + dy) % Y * CORES + c
        sem = u_y_s.at[dy - 1, 0] if sem is None else sem
        return remote(G.at[n, tp, m], G.at[n, tp, m], sem, u_y_r.at[dy - 1, u, m], ep, t)

    def unit_f(unit, dy, sem=None):
        G, n, u = unit
        t = (y - dy + Y) % Y * CORES + c
        sem = u_f_s.at[dy - 1, 0] if sem is None else sem
        return remote(G.at[n, t], G.at[n, t], sem, u_f_r.at[dy - 1, u], ep, partner)

    def unit_send_tile(unit, m):
        for dy in range(1, Y):
            y_sends[dy - 1].start(lambda sem: unit_y(unit, dy, m, sem))
        if m == tiles - 1:
            part_sends.start(lambda sem: unit_part(unit, sem))

    def unit_send(unit):
        for m in range(tiles):
            unit_send_tile(unit, m)

    def unit_forward(unit):
        for dy in range(1, Y):
            for m in range(tiles):
                unit_y(unit, dy, m).wait_recv()
            f_sends[dy - 1].start(lambda sem: unit_f(unit, dy, sem))

    def unit_dot(unit, w_ref):
        G, n = unit[:2]

        def pieces(ts):
            a = [G[n, t, m] for t in ts for m in range(tiles)]
            w = [w_ref[pl.ds(pl.multiple_of(t * width, width), width), :] for t in ts]
            return dot(jnp.concatenate(a, axis=1), jnp.concatenate(w, axis=0))

        unit_part(unit).wait_recv()
        chips = [(y - dy + Y) % Y for dy in range(1, Y)]
        out = pieces([tp, partner, *(chip * CORES + c for chip in chips)])
        for dy in range(1, Y):
            unit_f(unit, dy).wait_recv()
        return out + pieces([chip * CORES + 1 - c for chip in chips])

    shared_unit, own_unit = (GS, 0, 0), (GS, 1, 1)
    stages = (Z - 1) * CH
    stage_units = [(GE, n, 2 + n) for n in range(stages)]
    last_unit = (GL, 0, 2 + stages)
    head_units = [(GH, n, 3 + stages + n) for n in range(chunks)]

    def hidden(a, gate_w, up_w, unit):
        for m in range(tiles):
            at = slice(m * tile, (m + 1) * tile)
            h = silu(dot(a, gate_w[:, at])) * dot(a, up_w[:, at])
            unit[0][unit[1], tp, m] = h.astype(bf16)
            unit_send_tile(unit, m)

    def send_result(n, h):
        result_sends.start(
            lambda sem: remote(RO.at[n, h], RI.at[ep, h], sem, res_r.at[ep, h], order[n], tp)
        )

    row = lax.broadcasted_iota(jnp.int32, (BLOCK, BLOCK), 0)
    col = lax.broadcasted_iota(jnp.int32, (BLOCK, BLOCK), 1)
    causal = row >= col
    tril = causal.astype(f32)

    def scan_turn(n, _):
        at = pl.ds(pl.multiple_of(n * BLOCK, BLOCK), BLOCK)
        r = r_ref[at, :].astype(f32)
        log_sig = jnp.minimum(r, 0.0) - jnp.log1p(jnp.exp(-jnp.abs(r)))
        rate = log_sig / switch_softness + b_ref[at, :]
        inner = jnp.dot(tril, rate, precision=lax.Precision.HIGHEST, preferred_element_type=f32)
        last = inner[BLOCK - 1 : BLOCK, :]
        q = q_ref[at, :].astype(f32) * DK**-0.5
        k = k_ref[at, :].astype(f32)
        q_in = q * jnp.exp(inner)
        q_b = q_in.astype(bf16)
        k_b = (k * jnp.exp(-inner)).astype(bf16)
        k_out = (k * jnp.exp(last - inner)).astype(bf16)
        prior = state_ref[DV : DV + 1, :]
        far_ref[at, :] = (q * jnp.exp(inner + prior)).astype(bf16)
        entering = state_ref[0:DV, :]
        entering_b = entering.astype(bf16)
        updates = []
        for h in range(heads):
            ks = slice(h * DK, (h + 1) * DK)
            vs = slice(h * DV, (h + 1) * DV)
            v = v_ref[at, vs]
            scores = lax.dot_general(q_b[:, ks], k_b[:, ks], NT, preferred_element_type=f32)
            scores = jnp.where(causal, scores, 0.0).astype(bf16)
            out = jnp.dot(scores, v, preferred_element_type=f32)
            out += lax.dot_general(q_b[:, ks], entering_b[:, ks], NT, preferred_element_type=f32)
            mixed_ref[at, vs] = out
            updates.append(lax.dot_general(v, k_out[:, ks], TN, preferred_element_type=f32))
        state_ref[0:DV, :] = entering * jnp.exp(last) + jnp.concatenate(updates, axis=1)
        state_ref[DV : DV + 1, :] = prior + last
        return 0

    def put_state(dst, n):
        fade = state_ref[DV : DV + 8, :]
        high = fade.astype(bf16)
        low = (fade - high.astype(f32)).astype(bf16)
        dst[n, 0:DV, :] = state_ref[0:DV, :].astype(bf16)
        dst[n, DV : DV + PAD, :] = jnp.concatenate([high, low], axis=0)

    def state_a(dx):
        return remote(A.at[x], A.at[x], a_s.at[dx - 1], a_r.at[dx - 1], z * X + (x + dx) % X, tp)

    def state_b():
        return remote(B.at[0], B.at[1], b_s.at[0], b_r.at[0], (ep + X) % E, tp)

    def fold(src, n, state):
        fade = src[n, DV : DV + PAD, :].astype(f32)
        fade = fade[0:8] + fade[8:16]
        return fade, jnp.exp(fade[0:1]) * state + src[n, 0:DV, :].astype(f32)

    def combine():
        for dx in range(1, X):
            state_a(dx).wait_recv()
        state = jnp.zeros((DV, kw), f32)
        total = jnp.zeros((8, kw), f32)
        for n in range(X):
            fade, state = fold(A, n, state)
            total += fade
        state_ref[0:DV, :] = state
        state_ref[DV : DV + 8, :] = total
        enter_ref[...] = jnp.zeros_like(enter_ref)

    def chain(n):
        @pl.when(z == n)
        def _():
            if n:
                state_b().wait_recv()
                enter_ref[...] = B[1].astype(f32)
            if n < Z - 1:
                through = jnp.exp(state_ref[DV : DV + 1, :]) * enter_ref[...] + state_ref[0:DV, :]
                B[0] = through.astype(bf16)
                state_b().start()

    def enter():
        for n in range(X - 1):
            state = enter_ref[...]
            enter_ref[...] = jnp.where(n < x, fold(A, n, state)[1], state)

    def finish(i):
        at = pl.ds(i * rows, rows)
        state = enter_ref[...].astype(bf16)
        gain = gain_ref[...]
        for h in range(heads):
            ks = slice(h * DK, (h + 1) * DK)
            vs = slice(h * DV, (h + 1) * DV)
            m = mixed_ref[at, vs] + lax.dot_general(
                far_ref[at, ks], state[:, ks], NT, preferred_element_type=f32
            )
            scale = lax.rsqrt(jnp.mean(m * m, axis=-1, keepdims=True) + eps_norm)
            gate = silu(og_ref[at, vs].astype(f32))
            at_tile = slice(h * DV % tile, h * DV % tile + DV)
            GH[i, tp, h * DV // tile, :, at_tile] = (m * scale * gain * gate).astype(bf16)

    order = [z * X + (x + dx) % X for dx in range(X)]
    for j in range(1, Z):
        order += [near(j) * X + (x + dx) % X for dx in range(X)]

    def expert_hidden(pieces, unit):
        for n, h in pieces:
            row_part(order[n], h).wait_recv()
        a = jnp.concatenate([rows_of(order[n], h) for n, h in pieces], axis=0)
        hidden(a, eg_ref, eu_ref, unit)

    def expert_result(pieces, unit, hold=None):
        out = unit_dot(unit, ed_ref).astype(bf16)
        size = part * CORES
        for i, (n, h) in enumerate(pieces):
            RO[n, h] = out[i * size : (i + 1) * size]
        for n, h in pieces:
            if n % X and hold is not None:
                hold.append((n, h))
            elif n:
                send_result(n, h)

    turns = seq // BLOCK

    def scan(lo, hi):
        lax.fori_loop(lo, hi, scan_turn, 0, unroll=hi - lo)

    for h in range(CH):
        send_own(h)
    own = jnp.concatenate([rows_of(ep, h) for h in range(CH)], axis=0)
    need(sg_ref, su_ref)
    hidden(own, sg_ref, su_ref, shared_unit)
    need(eg_ref, eu_ref)
    hidden(own, eg_ref, eu_ref, own_unit)
    need(r_ref, b_ref, q_ref, k_ref, v_ref)
    load(late)
    state_ref[...] = jnp.zeros_like(state_ref)
    own_pieces = [(0, h) for h in range(CH)]
    stage_pieces = []

    def states():
        put_state(A, x)
        for dx in range(1, X):
            state_a(dx).start()

    def shared_down():
        need(sd_ref)
        acc_ref[...] = unit_dot(shared_unit, sd_ref)
        need(ed_ref)
        expert_result(own_pieces, own_unit)

    def forward(unit):
        unit_forward(unit)

    def mixing(what):
        if what == 0:
            combine()
        chain(what)

    scan(0, turns // 2)
    fillers = {
        0: lambda: scan(turns // 2, 3 * turns // 4),
        1: lambda: (scan(3 * turns // 4, turns), states()),
    }
    held = []
    for n in range(stages):
        j, h = n // CH + 1, n % CH
        relay_line(j, h)
        for dx in range(1, X):
            relay_side(j - 1, h, dx)
        stage_pieces.append([((j - 1) * X + dx, h) for dx in range(1, X)] + [(j * X, h)])
        fillers.get(n, lambda: None)()
        if n >= 3:
            expert_result(stage_pieces[n - 3], stage_units[n - 3], held)
        if n == 1:
            forward(shared_unit)
            forward(own_unit)
        if n == 2:
            shared_down()
        expert_hidden(stage_pieces[n], stage_units[n])
        if n > stages - Z:
            mixing(n - (stages - Z) - 1)
        if n >= 2:
            forward(stage_units[n - 2])
    last_pieces = [((Z - 1) * X + dx, h) for dx in range(1, X) for h in range(CH)]
    for h in range(CH):
        for dx in range(1, X):
            relay_side(Z - 1, h, dx)
    for piece in held or ():
        send_result(*piece)
    expert_result(stage_pieces[stages - 3], stage_units[stages - 3])
    expert_hidden(last_pieces, last_unit)
    forward(stage_units[-2])
    mixing(Z - 1)
    need(og_ref, gain_ref)
    enter()
    for i in range(chunks // 2):
        finish(i)
        unit_send(head_units[i])
    expert_result(stage_pieces[-2], stage_units[-2])
    for i in range(chunks // 2, chunks):
        finish(i)
        unit_send(head_units[i])
    forward(stage_units[-1])
    expert_result(stage_pieces[-1], stage_units[-1])
    need(wo_ref)
    need(idx_ref, w_ref)

    index, given = idx_ref[...], w_ref[...]
    by_expert = [jnp.sum(jnp.where(index == e, given, 0.0), axis=0, keepdims=True) for e in range(E)]
    by_expert = jnp.transpose(jnp.concatenate(by_expert, axis=0), (1, 0))
    lane = lax.broadcasted_iota(jnp.int32, by_expert.shape, 1)

    def weight(e):
        return jnp.sum(jnp.where(lane == e, by_expert, 0.0), axis=1, keepdims=True)

    def mixer(i):
        at = pl.ds(i * rows, rows)
        mixer_ref[at, :] = unit_dot(head_units[i], wo_ref).astype(bf16)

    order_weights = [weight(e) for e in order]

    def collect():
        for n in range(1, E):
            e = order[n]
            for h in range(CH):
                remote(RO.at[n, h], RI.at[e, h], res_s.at[0], res_r.at[e, h], e, tp).wait_recv()
        for h in range(CH):
            at = slice(h * (rows // CH), (h + 1) * (rows // CH))
            total = acc_ref[at] + RO[0, h].astype(f32) * order_weights[0][at]
            for n in range(1, E):
                total += RI[order[n], h].astype(f32) * order_weights[n][at]
            blend_ref[at, :] = total.astype(bf16)

    forward(last_unit)
    expert_result(last_pieces, last_unit)
    for i in range(chunks):
        forward(head_units[i])
        mixer(i)
    collect()

    for h in range(CH):
        pl.when(z < Z - 1)(lambda: row_up(ep, h).wait_send())
        pl.when(z > 0)(lambda: row_down(ep, h, r_down_s.at[h]).wait_send())
        for k in range(1, Z):
            pl.when((z >= k) & (z < Z - 1))(lambda: row_up(ep - k * X, h).wait_send())
            pl.when((z + k < Z) & (z > 0))(lambda: row_down(ep + k * X, h).wait_send())
        for dx in range(1, X):
            kind = 2 + (dx - 1) * (Z + 2)
            row_x(ep, h, dx).wait_send()
            row_part(ep, h, kind).wait_send()
            for k in range(1, Z):
                zk = near(k)
                pl.when(by_x(zk, h))(lambda: row_x(zk * X + x, h, dx).wait_send())
                pl.when((zk > 0) & (zk < Z - 1))(lambda: row_part(ep, h, kind + k).wait_send())
            pl.when(z < Z - 1)(lambda: row_part(ep, h, kind + Z).wait_send())
            pl.when(z > 0)(lambda: row_part(ep, h, kind + Z + 1).wait_send())
            pl.when(z < Z - 1 - spare(h))(lambda: side_row(ep, h, True, dx).wait_send())
            pl.when(z > spare(h))(lambda: side_row(ep, h, False, dx).wait_send())
        pl.when(z > 0)(lambda: row_part(ep, h, 0).wait_send())
        pl.when(z < Z - 1)(lambda: row_part(ep, h, 1).wait_send())
    for sends in (part_sends, *y_sends, *f_sends, result_sends):
        sends.drain()
    for dx in range(1, X):
        state_a(dx).wait_send()
    pl.when(z < Z - 1)(lambda: state_b().wait_send())


def local(
    queries,
    sequence_keys,
    stream_content_vectors,
    output_gate_logits,
    retention_preactivation,
    additional_fade_bias,
    attention_group_rescale,
    output_projection,
    expert_batch_tokens,
    expert_norm_gain,
    routed_expert_index,
    routed_expert_weights,
    expert_gate_matrix,
    expert_up_matrix,
    expert_down_matrix,
    shared_gate_matrix,
    shared_up_matrix,
    shared_down_matrix,
):
    experts, lanes = lax.axis_size("ep"), lax.axis_size("tp")
    X = 2 ** (int(math.log2(experts)) // 2)
    Z, Y = experts // X, lanes // CORES
    rows, model_width = expert_batch_tokens.shape
    seq, kw = queries.shape
    vw = stream_content_vectors.shape[1]
    width = shared_gate_matrix.shape[1]
    chunks = seq // rows
    stages = (Z - 1) * CH
    units = 3 + stages + chunks
    tile = min(256, width)
    tiles = width // tile
    args = (
        queries,
        sequence_keys,
        stream_content_vectors,
        output_gate_logits,
        retention_preactivation,
        additional_fade_bias,
        attention_group_rescale.reshape(1, DV),
        output_projection,
        expert_batch_tokens,
        expert_norm_gain.reshape(1, model_width),
        routed_expert_index.T,
        routed_expert_weights.T,
        expert_gate_matrix[0],
        expert_up_matrix[0],
        expert_down_matrix[0],
        shared_gate_matrix,
        shared_up_matrix,
        shared_down_matrix,
    )
    outs = (
        jax.ShapeDtypeStruct((seq, output_projection.shape[1]), bf16),
        jax.ShapeDtypeStruct((rows, shared_down_matrix.shape[1]), bf16),
    )
    dma = lambda *shape: pltpu.SemaphoreType.DMA(shape)
    scratch = [pltpu.VMEM(a.shape, a.dtype) for a in args]
    scratch += [
        pltpu.VMEM((experts, CH, CORES, rows // (CH * CORES), model_width), bf16),
        pltpu.VMEM((2, lanes, tiles, rows, tile), bf16),
        pltpu.VMEM((stages, lanes, tiles, X * rows // CH, tile), bf16),
        pltpu.VMEM((1, lanes, tiles, (X - 1) * rows, tile), bf16),
        pltpu.VMEM((chunks, lanes, tiles, rows, tile), bf16),
        pltpu.VMEM((experts, CH, rows // CH, outs[1].shape[1]), bf16),
        pltpu.VMEM((experts, CH, rows // CH, outs[1].shape[1]), bf16),
        pltpu.VMEM((X, DV + PAD, kw), bf16),
        pltpu.VMEM((2, DV, kw), bf16),
        pltpu.VMEM((seq, vw), f32),
        pltpu.VMEM((seq, kw), bf16),
        pltpu.VMEM((DV + 8, kw), f32),
        pltpu.VMEM((DV, kw), f32),
        pltpu.VMEM((rows, outs[1].shape[1]), f32),
        dma(11),
        dma(2 + (X - 1) * (Z + 2), CH),
        dma(Z, CH),
        dma(CH),
        dma(X - 1, Z, CH),
        dma(X - 1, 2, CH),
        dma(experts, CH),
        dma(experts, CH),
        dma(5),
        dma(units),
        dma(Y - 1, 9 * tiles),
        dma(Y - 1, units, tiles),
        dma(Y - 1, 3),
        dma(Y - 1, units),
        dma(14),
        dma(experts, CH),
        dma(X - 1),
        dma(X - 1),
        dma(1),
        dma(1),
    ]
    made = pl.pallas_call(
        functools.partial(body, (Z, X, Y)),
        out_shape=tuple(pltpu.VMEM(o.shape, o.dtype) for o in outs),
        in_specs=[pl.BlockSpec(memory_space=pl.ANY)] * len(args),
        out_specs=tuple([pl.BlockSpec(memory_space=pltpu.VMEM)] * len(outs)),
        scratch_shapes=scratch,
        compiler_params=pltpu.CompilerParams(
            collective_id=0, has_side_effects=True, vmem_limit_bytes=66000000
        ),
        cost_estimate=pl.CostEstimate(
            flops=10**10, bytes_accessed=20 * 2**20, transcendentals=10**6
        ),
        name="step",
    )(*args)
    return pl.pallas_call(
        settle,
        out_shape=outs,
        in_specs=[pl.BlockSpec(memory_space=pltpu.VMEM)] * 2,
        out_specs=tuple([pl.BlockSpec(memory_space=pl.ANY)] * 2),
        scratch_shapes=[dma(2)],
        cost_estimate=pl.CostEstimate(flops=10**6, bytes_accessed=2**21, transcendentals=0),
        name="settle",
    )(*[pltpu.with_memory_space_constraint(m, pltpu.VMEM) for m in made])


def settle(mixer_ref, blend_ref, mixer_out, blend_out, sem):
    writes = [
        pltpu.make_async_copy(mixer_ref, mixer_out, sem.at[0]),
        pltpu.make_async_copy(blend_ref, blend_out, sem.at[1]),
    ]
    for copy in writes:
        copy.start()
    for copy in writes:
        copy.wait()


def solution(mesh):
    in_specs = (
        P("ep", "tp"),
        P("ep", "tp"),
        P("ep", "tp"),
        P("ep", "tp"),
        P("ep", "tp"),
        P("ep", "tp"),
        P(),
        P(None, "tp"),
        P("ep", None),
        P(),
        P("ep", None),
        P("ep", None),
        P("ep", None, "tp"),
        P("ep", None, "tp"),
        P("ep", None, "tp"),
        P(None, "tp"),
        P(None, "tp"),
        P(None, "tp"),
    )
    out_specs = (P("ep", "tp"), P("ep", "tp"))
    return jax.shard_map(local, mesh=mesh, in_specs=in_specs, out_specs=out_specs, check_vma=False)
```

```python
import functools
import math

import jax
import jax.numpy as jnp
from jax import lax
from jax.experimental import pallas as pl
from jax.experimental.pallas import tpu as pltpu
from jax.sharding import PartitionSpec as P

DK = 64
DV = 128
BLOCK = 64
PAD = 16
CORES = 2
CH = 2

eps_norm = 1e-06
switch_softness = 16.0
bf16 = jnp.bfloat16
f32 = jnp.float32
NT = (((1,), (1,)), ((), ()))
TN = (((0,), (0,)), ((), ()))
MESH = pl.DeviceIdType.MESH


def silu(x):
    return x * jax.nn.sigmoid(x)


def dot(a, b):
    return jnp.dot(a, b, preferred_element_type=f32)


def body(sizes, *refs):
    Z, X, Y = sizes
    E = Z * X
    (
        q_hbm, k_hbm, v_hbm, og_hbm, r_hbm, b_hbm, gain_hbm, wo_hbm, tok_hbm, ng_hbm, idx_hbm, w_hbm,
        eg_hbm, eu_hbm, ed_hbm, sg_hbm, su_hbm, sd_hbm,
        mixer_ref, blend_ref,
        q_ref, k_ref, v_ref, og_ref, r_ref, b_ref, gain_ref, wo_ref, tok_ref, ng_ref, idx_ref, w_ref,
        eg_ref, eu_ref, ed_ref, sg_ref, su_ref, sd_ref,
        R, GS, GE, GL, GH, RO, RI, A, B, mixed_ref, far_ref, state_ref, enter_ref, acc_ref,
        in_sem,
        r_part_s, r_z_s, r_down_s, r_x_s, r_side_s, r_far_r, r_part_r,
        u_part_s, u_part_r, u_y_s, u_y_r, u_f_s, u_f_r,
        res_s, res_r, a_s, a_r, b_s, b_r,
    ) = refs

    ep, tp = lax.axis_index("ep"), lax.axis_index("tp")
    z, x = ep // X, ep % X
    y, c = tp // CORES, tp % CORES
    partner = y * CORES + (1 - c)
    rows = tok_ref.shape[0]
    seq, kw = q_ref.shape
    heads = kw // DK
    chunks = seq // rows
    tiles, tile = GS.shape[2], GS.shape[-1]
    width = tiles * tile
    part = rows // (CH * CORES)

    def remote(src, dst, ssem, rsem, e, t):
        return pltpu.make_async_remote_copy(
            src_ref=src,
            dst_ref=dst,
            send_sem=ssem,
            recv_sem=rsem,
            device_id={"ep": e, "tp": t},
            device_id_type=MESH,
        )

    early = [
        (tok_hbm, tok_ref), (ng_hbm, ng_ref), (sg_hbm, sg_ref), (su_hbm, su_ref), (eg_hbm, eg_ref), (eu_hbm, eu_ref),
        (r_hbm, r_ref), (b_hbm, b_ref), (q_hbm, q_ref), (k_hbm, k_ref), (v_hbm, v_ref),
    ]
    late = [
        (sd_hbm, sd_ref), (ed_hbm, ed_ref), (og_hbm, og_ref), (gain_hbm, gain_ref), (wo_hbm, wo_ref),
        (idx_hbm, idx_ref), (w_hbm, w_ref),
    ]
    copies = {}

    def load(pairs, first=0):
        for n, (src, dst) in enumerate(pairs, first):
            copies[id(dst)] = pltpu.make_async_copy(src, dst, in_sem.at[n])
            copies[id(dst)].start()

    load(early[:2])

    barrier = pltpu.get_barrier_semaphore()

    def greet(e, t):
        pl.semaphore_signal(barrier, inc=1, device_id={"ep": e, "tp": t}, device_id_type=MESH)

    greet(ep, partner)
    for dy in range(1, Y):
        greet(ep, (y + dy) % Y * CORES + c)
    for dx in range(1, X):
        greet(z * X + (x + dx) % X, tp)
    pl.when(z < Z - 1)(lambda: greet(ep + X, tp))
    pl.when(z > 0)(lambda: greet(ep - X, tp))

    load(early[2:], 2)

    def need(*dsts):
        for dst in dsts:
            copies[id(dst)].wait()

    class Sends:
        def __init__(self, sems, count):
            self.sems, self.count, self.sent, self.held = sems, count, 0, {}

        def start(self, make):
            n = self.sent % self.count
            if n in self.held:
                self.held[n].wait_send()
            self.held[n] = make(self.sems.at[n])
            self.held[n].start()
            self.sent += 1

        def drain(self):
            for copy in self.held.values():
                copy.wait_send()

    need(tok_ref, ng_ref)
    flat = tok_ref[...].astype(f32)
    normed = (
        flat * lax.rsqrt(jnp.mean(flat * flat, axis=-1, keepdims=True) + eps_norm) * ng_ref[...]
    ).astype(bf16)
    for n in range(CH * CORES):
        R[ep, n // CORES, n % CORES] = normed[n * part : (n + 1) * part]

    lines = jnp.where(z < Z - 1, 1, 0) + jnp.where(z > 0, 1, 0)
    pl.semaphore_wait(barrier, 1 + (Y - 1) + (X - 1) + lines)

    def row_part(b, h, kind=0):
        return remote(R.at[b, h, c], R.at[b, h, c], r_part_s.at[kind, h], r_part_r.at[b, h], ep, partner)

    def row_up(b, h):
        return remote(R.at[b, h, c], R.at[b, h, c], r_z_s.at[b // X, h], r_far_r.at[b, h], ep + X, tp)

    def row_down(b, h, sem=None):
        sem = r_z_s.at[b // X, h] if sem is None else sem
        return remote(R.at[b, h, c], R.at[b, h, c], sem, r_far_r.at[b, h], ep - X, tp)

    def row_x(b, h, dx):
        there = z * X + (x + dx) % X
        return remote(R.at[b, h, c], R.at[b, h, c], r_x_s.at[dx - 1, b // X, h], r_far_r.at[b, h], there, tp)

    def near(j):
        up = jnp.where(j <= Z - 1 - z, z + j, Z - 1 - j)
        down = jnp.where(j <= z, z - j, j)
        return jnp.where(2 * z < Z, up, down)

    def send_own(h):
        pl.when(z < Z - 1)(lambda: row_up(ep, h).start())
        pl.when(z > 0)(lambda: row_down(ep, h, r_down_s.at[h]).start())
        for dx in range(1, X):
            row_x(ep, h, dx).start()

    def arrive(b, h):
        remote(R.at[b, h, c], R.at[b, h, c], r_part_s.at[0, h], r_far_r.at[b, h], ep, partner).wait_recv()

    def hand_over(b, h, kind, again):
        copy = row_part(b, h, kind)
        if again:
            copy.wait_send()
        copy.start()

    def relay_line(k, h):
        @pl.when(z >= k)
        def _():
            b = ep - k * X
            arrive(b, h)
            pl.when(z < Z - 1)(lambda: row_up(b, h).start())
            hand_over(b, h, 0, k > 1)

        @pl.when(z + k < Z)
        def _():
            b = ep + k * X
            arrive(b, h)
            pl.when(z > 0)(lambda: row_down(b, h).start())
            hand_over(b, h, 1, k > 1)

        @pl.when(by_x(near(k), h))
        def _():
            for dx in range(1, X):
                row_x(near(k) * X + x, h, dx).start()

    def by_x(zj, h):
        use = (zj > 0) & (zj < Z - 1)
        if h == CH - 1:
            use |= (zj + z == Z - 1) & ((z == 0) | (z == Z - 1))
        return use

    def spare(h):
        return 1 if h == CH - 1 else 0

    def side(j, dx):
        return near(j) * X + (x + dx) % X

    def top(dx):
        return (Z - 1) * X + (x + dx) % X

    def bottom(dx):
        return (x + dx) % X

    def side_row(b, h, up, dx):
        there = ep + X if up else ep - X
        sem = r_side_s.at[dx - 1, int(up), h]
        return remote(R.at[b, h, c], R.at[b, h, c], sem, r_far_r.at[b, h], there, tp)

    def relay_side(j, h, dx):
        kind = 2 + (dx - 1) * (Z + 2)

        def here(b, n):
            arrive(b, h)
            row_part(b, h, kind + n).start()

        if j == 0:
            here(side(0, dx), 0)
            pl.when(z == 0)(lambda: side_row(bottom(dx), h, True, dx).start())
            pl.when(z == Z - 1)(lambda: side_row(top(dx), h, False, dx).start())
            return

        pl.when((near(j) > 0) & (near(j) < Z - 1))(lambda: here(side(j, dx), j))

        @pl.when(z == Z - 1 - j)
        def _():
            here(top(dx), Z)
            pl.when(z > spare(h))(lambda: side_row(top(dx), h, False, dx).start())

        @pl.when(z == j)
        def _():
            here(bottom(dx), Z + 1)
            pl.when(z < Z - 1 - spare(h))(lambda: side_row(bottom(dx), h, True, dx).start())

    def rows_of(b, h):
        return jnp.concatenate([R[b, h, n] for n in range(CORES)], axis=0)

    heads_from = 3 + (Z - 1) * CH
    part_sends = Sends(u_part_s, u_part_s.shape[0])
    y_sends = [Sends(u_y_s.at[n], u_y_s.shape[1]) for n in range(Y - 1)]
    f_sends = [Sends(u_f_s.at[n], u_f_s.shape[1]) for n in range(Y - 1)]
    result_sends = Sends(res_s, res_s.shape[0])

    def unit_part(unit, sem=None):
        G, n, u = unit
        sem = u_part_s.at[0] if sem is None else sem
        return remote(G.at[n, tp], G.at[n, tp], sem, u_part_r.at[u], ep, partner)

    def unit_y(unit, dy, m, sem=None):
        G, n, u = unit
        t = (y + dy) % Y * CORES + c
        sem = u_y_s.at[dy - 1, 0] if sem is None else sem
        piece = G.at[n, tp] if messages(unit) == 1 else G.at[n, tp, m]
        return remote(piece, piece, sem, u_y_r.at[dy - 1, slot_of(u, m)], ep, t)

    def slot_of(u, m):
        return u * tiles + m if u < heads_from else heads_from * (tiles - 1) + u

    def messages(unit):
        return tiles if unit[2] < heads_from else 1

    def unit_f(unit, dy, sem=None):
        G, n, u = unit
        t = (y - dy + Y) % Y * CORES + c
        sem = u_f_s.at[dy - 1, 0] if sem is None else sem
        return remote(G.at[n, t], G.at[n, t], sem, u_f_r.at[dy - 1, u], ep, partner)

    def unit_send_tile(unit, m):
        for dy in range(1, Y):
            y_sends[dy - 1].start(lambda sem: unit_y(unit, dy, m, sem))
        if m == messages(unit) - 1:
            part_sends.start(lambda sem: unit_part(unit, sem))

    def unit_send(unit):
        for m in range(messages(unit)):
            unit_send_tile(unit, m)

    def unit_forward(unit):
        for dy in range(1, Y):
            for m in range(messages(unit)):
                unit_y(unit, dy, m).wait_recv()
            f_sends[dy - 1].start(lambda sem: unit_f(unit, dy, sem))

    def unit_dot(unit, w_ref):
        G, n = unit[:2]

        def pieces(ts):
            a = [G[n, t, m] for t in ts for m in range(tiles)]
            w = [w_ref[pl.ds(pl.multiple_of(t * width, width), width), :] for t in ts]
            return dot(jnp.concatenate(a, axis=1), jnp.concatenate(w, axis=0))

        unit_part(unit).wait_recv()
        chips = [(y - dy + Y) % Y for dy in range(1, Y)]
        out = pieces([tp, partner, *(chip * CORES + c for chip in chips)])
        for dy in range(1, Y):
            unit_f(unit, dy).wait_recv()
        return out + pieces([chip * CORES + 1 - c for chip in chips])

    shared_unit, own_unit = (GS, 0, 0), (GS, 1, 1)
    stages = (Z - 1) * CH
    stage_units = [(GE, n, 2 + n) for n in range(stages)]
    last_unit = (GL, 0, 2 + stages)
    head_units = [(GH, n, 3 + stages + n) for n in range(chunks)]

    def hidden(a, gate_w, up_w, unit):
        for m in range(tiles):
            at = slice(m * tile, (m + 1) * tile)
            h = silu(dot(a, gate_w[:, at])) * dot(a, up_w[:, at])
            unit[0][unit[1], tp, m] = h.astype(bf16)
            unit_send_tile(unit, m)

    def send_result(n, h):
        result_sends.start(
            lambda sem: remote(RO.at[n, h], RI.at[ep, h], sem, res_r.at[ep], order[n], tp)
        )

    def send_whole_result(n):
        result_sends.start(lambda sem: remote(RO.at[n], RI.at[ep], sem, res_r.at[ep], order[n], tp))

    row = lax.broadcasted_iota(jnp.int32, (BLOCK, BLOCK), 0)
    col = lax.broadcasted_iota(jnp.int32, (BLOCK, BLOCK), 1)
    causal = row >= col
    tril = causal.astype(f32)

    def scan_turn(n, _):
        at = pl.ds(pl.multiple_of(n * BLOCK, BLOCK), BLOCK)
        r = r_ref[at, :].astype(f32)
        log_sig = jnp.minimum(r, 0.0) - jnp.log1p(jnp.exp(-jnp.abs(r)))
        rate = log_sig / switch_softness + b_ref[at, :]
        inner = jnp.dot(tril, rate, precision=lax.Precision.HIGHEST, preferred_element_type=f32)
        last = inner[BLOCK - 1 : BLOCK, :]
        q = q_ref[at, :].astype(f32) * DK**-0.5
        k = k_ref[at, :].astype(f32)
        q_in = q * jnp.exp(inner)
        q_b = q_in.astype(bf16)
        k_b = (k * jnp.exp(-inner)).astype(bf16)
        k_out = (k * jnp.exp(last - inner)).astype(bf16)
        prior = state_ref[DV : DV + 1, :]
        far_ref[at, :] = (q * jnp.exp(inner + prior)).astype(bf16)
        entering = state_ref[0:DV, :]
        entering_b = entering.astype(bf16)
        updates = []
        for h in range(heads):
            ks = slice(h * DK, (h + 1) * DK)
            vs = slice(h * DV, (h + 1) * DV)
            v = v_ref[at, vs]
            scores = lax.dot_general(q_b[:, ks], k_b[:, ks], NT, preferred_element_type=f32)
            scores = jnp.where(causal, scores, 0.0).astype(bf16)
            out = jnp.dot(scores, v, preferred_element_type=f32)
            out += lax.dot_general(q_b[:, ks], entering_b[:, ks], NT, preferred_element_type=f32)
            mixed_ref[at, vs] = out
            updates.append(lax.dot_general(v, k_out[:, ks], TN, preferred_element_type=f32))
        state_ref[0:DV, :] = entering * jnp.exp(last) + jnp.concatenate(updates, axis=1)
        state_ref[DV : DV + 1, :] = prior + last
        return 0

    def put_state(dst, n):
        fade = state_ref[DV : DV + 8, :]
        high = fade.astype(bf16)
        low = (fade - high.astype(f32)).astype(bf16)
        dst[n, 0:DV, :] = state_ref[0:DV, :].astype(bf16)
        dst[n, DV : DV + PAD, :] = jnp.concatenate([high, low], axis=0)

    def state_a(dx):
        return remote(A.at[x], A.at[x], a_s.at[dx - 1], a_r.at[dx - 1], z * X + (x + dx) % X, tp)

    def state_b():
        return remote(B.at[0], B.at[1], b_s.at[0], b_r.at[0], (ep + X) % E, tp)

    def fold(src, n, state):
        fade = src[n, DV : DV + PAD, :].astype(f32)
        fade = fade[0:8] + fade[8:16]
        return fade, jnp.exp(fade[0:1]) * state + src[n, 0:DV, :].astype(f32)

    def combine():
        for dx in range(1, X):
            state_a(dx).wait_recv()
        state = jnp.zeros((DV, kw), f32)
        total = jnp.zeros((8, kw), f32)
        for n in range(X):
            fade, state = fold(A, n, state)
            total += fade
        state_ref[0:DV, :] = state
        state_ref[DV : DV + 8, :] = total
        enter_ref[...] = jnp.zeros_like(enter_ref)

    def chain(n):
        @pl.when(z == n)
        def _():
            if n:
                state_b().wait_recv()
                enter_ref[...] = B[1].astype(f32)
            if n < Z - 1:
                through = jnp.exp(state_ref[DV : DV + 1, :]) * enter_ref[...] + state_ref[0:DV, :]
                B[0] = through.astype(bf16)
                state_b().start()

    def enter():
        for n in range(X - 1):
            state = enter_ref[...]
            enter_ref[...] = jnp.where(n < x, fold(A, n, state)[1], state)

    def finish(i):
        at = pl.ds(i * rows, rows)
        state = enter_ref[...].astype(bf16)
        gain = gain_ref[...]
        for h in range(heads):
            ks = slice(h * DK, (h + 1) * DK)
            vs = slice(h * DV, (h + 1) * DV)
            m = mixed_ref[at, vs] + lax.dot_general(
                far_ref[at, ks], state[:, ks], NT, preferred_element_type=f32
            )
            scale = lax.rsqrt(jnp.mean(m * m, axis=-1, keepdims=True) + eps_norm)
            gate = silu(og_ref[at, vs].astype(f32))
            at_tile = slice(h * DV % tile, h * DV % tile + DV)
            GH[i, tp, h * DV // tile, :, at_tile] = (m * scale * gain * gate).astype(bf16)

    order = [z * X + (x + dx) % X for dx in range(X)]
    for j in range(1, Z):
        order += [near(j) * X + (x + dx) % X for dx in range(X)]

    def expert_hidden(pieces, unit):
        for n, h in pieces:
            row_part(order[n], h).wait_recv()
        a = jnp.concatenate([rows_of(order[n], h) for n, h in pieces], axis=0)
        hidden(a, eg_ref, eu_ref, unit)

    def expert_result(pieces, unit, hold=None, whole=False):
        out = unit_dot(unit, ed_ref).astype(bf16)
        size = part * CORES
        for i, (n, h) in enumerate(pieces):
            RO[n, h] = out[i * size : (i + 1) * size]
        if whole:
            for n in sorted({n for n, _ in pieces}):
                send_whole_result(n)
            return
        for n, h in pieces:
            if n % X and hold is not None:
                hold.append((n, h))
            elif n:
                send_result(n, h)

    turns = seq // BLOCK

    def scan(lo, hi):
        lax.fori_loop(lo, hi, scan_turn, 0, unroll=hi - lo)

    for h in range(CH):
        send_own(h)
    own = jnp.concatenate([rows_of(ep, h) for h in range(CH)], axis=0)
    need(sg_ref, su_ref)
    hidden(own, sg_ref, su_ref, shared_unit)
    need(eg_ref, eu_ref)
    hidden(own, eg_ref, eu_ref, own_unit)
    need(r_ref, b_ref, q_ref, k_ref, v_ref)
    load(late)
    state_ref[...] = jnp.zeros_like(state_ref)
    own_pieces = [(0, h) for h in range(CH)]
    stage_pieces = []

    def states():
        put_state(A, x)
        for dx in range(1, X):
            state_a(dx).start()

    def shared_down():
        need(sd_ref)
        acc_ref[...] = unit_dot(shared_unit, sd_ref)
        need(ed_ref)
        expert_result(own_pieces, own_unit)

    def forward(unit):
        unit_forward(unit)

    def mixing(what):
        if what == 0:
            combine()
        chain(what)

    scan(0, turns // 2)
    fillers = {
        0: lambda: scan(turns // 2, 3 * turns // 4),
        1: lambda: (scan(3 * turns // 4, turns), states()),
    }
    held = []
    for n in range(stages):
        j, h = n // CH + 1, n % CH
        relay_line(j, h)
        for dx in range(1, X):
            relay_side(j - 1, h, dx)
        stage_pieces.append([((j - 1) * X + dx, h) for dx in range(1, X)] + [(j * X, h)])
        fillers.get(n, lambda: None)()
        if n >= 3:
            expert_result(stage_pieces[n - 3], stage_units[n - 3], held)
        if n == 1:
            forward(shared_unit)
            forward(own_unit)
        if n == 2:
            shared_down()
        expert_hidden(stage_pieces[n], stage_units[n])
        if n > stages - Z:
            mixing(n - (stages - Z) - 1)
        if n >= 2:
            forward(stage_units[n - 2])
    last_pieces = [((Z - 1) * X + dx, h) for dx in range(1, X) for h in range(CH)]
    for h in range(CH):
        for dx in range(1, X):
            relay_side(Z - 1, h, dx)
    for n, h in held:
        if all((n, m) in held for m in range(CH)):
            if h == 0:
                send_whole_result(n)
        else:
            send_result(n, h)
    expert_result(stage_pieces[stages - 3], stage_units[stages - 3])
    expert_hidden(last_pieces, last_unit)
    forward(stage_units[-2])
    mixing(Z - 1)
    need(og_ref, gain_ref)
    enter()
    for i in range(chunks // 2):
        finish(i)
        unit_send(head_units[i])
    expert_result(stage_pieces[-2], stage_units[-2])
    forward(stage_units[-1])
    for i in range(chunks // 2, chunks):
        finish(i)
        unit_send(head_units[i])
    expert_result(stage_pieces[-1], stage_units[-1])
    need(wo_ref)
    need(idx_ref, w_ref)

    index, given = idx_ref[...], w_ref[...]
    by_expert = [jnp.sum(jnp.where(index == e, given, 0.0), axis=0, keepdims=True) for e in range(E)]
    by_expert = jnp.transpose(jnp.concatenate(by_expert, axis=0), (1, 0))
    lane = lax.broadcasted_iota(jnp.int32, by_expert.shape, 1)

    def weight(e):
        return jnp.sum(jnp.where(lane == e, by_expert, 0.0), axis=1, keepdims=True)

    def mixer(i):
        at = pl.ds(i * rows, rows)
        mixer_ref[at, :] = unit_dot(head_units[i], wo_ref).astype(bf16)

    order_weights = [weight(e) for e in order]

    def collect():
        for n in range(1, E):
            e = order[n]
            remote(RO.at[n], RI.at[e], res_s.at[0], res_r.at[e], e, tp).wait_recv()
        for h in range(CH):
            at = slice(h * (rows // CH), (h + 1) * (rows // CH))
            total = acc_ref[at] + RO[0, h].astype(f32) * order_weights[0][at]
            for n in range(1, E):
                total += RI[order[n], h].astype(f32) * order_weights[n][at]
            blend_ref[at, :] = total.astype(bf16)

    forward(last_unit)
    expert_result(last_pieces, last_unit, whole=True)
    for i in range(chunks):
        forward(head_units[i])
        mixer(i)
    collect()

    for h in range(CH):
        pl.when(z < Z - 1)(lambda: row_up(ep, h).wait_send())
        pl.when(z > 0)(lambda: row_down(ep, h, r_down_s.at[h]).wait_send())
        for k in range(1, Z):
            pl.when((z >= k) & (z < Z - 1))(lambda: row_up(ep - k * X, h).wait_send())
            pl.when((z + k < Z) & (z > 0))(lambda: row_down(ep + k * X, h).wait_send())
        for dx in range(1, X):
            kind = 2 + (dx - 1) * (Z + 2)
            row_x(ep, h, dx).wait_send()
            row_part(ep, h, kind).wait_send()
            for k in range(1, Z):
                zk = near(k)
                pl.when(by_x(zk, h))(lambda: row_x(zk * X + x, h, dx).wait_send())
                pl.when((zk > 0) & (zk < Z - 1))(lambda: row_part(ep, h, kind + k).wait_send())
            pl.when(z < Z - 1)(lambda: row_part(ep, h, kind + Z).wait_send())
            pl.when(z > 0)(lambda: row_part(ep, h, kind + Z + 1).wait_send())
            pl.when(z < Z - 1 - spare(h))(lambda: side_row(ep, h, True, dx).wait_send())
            pl.when(z > spare(h))(lambda: side_row(ep, h, False, dx).wait_send())
        pl.when(z > 0)(lambda: row_part(ep, h, 0).wait_send())
        pl.when(z < Z - 1)(lambda: row_part(ep, h, 1).wait_send())
    for sends in (part_sends, *y_sends, *f_sends, result_sends):
        sends.drain()
    for dx in range(1, X):
        state_a(dx).wait_send()
    pl.when(z < Z - 1)(lambda: state_b().wait_send())


def local(
    queries,
    sequence_keys,
    stream_content_vectors,
    output_gate_logits,
    retention_preactivation,
    additional_fade_bias,
    attention_group_rescale,
    output_projection,
    expert_batch_tokens,
    expert_norm_gain,
    routed_expert_index,
    routed_expert_weights,
    expert_gate_matrix,
    expert_up_matrix,
    expert_down_matrix,
    shared_gate_matrix,
    shared_up_matrix,
    shared_down_matrix,
):
    experts, lanes = lax.axis_size("ep"), lax.axis_size("tp")
    X = 2 ** (int(math.log2(experts)) // 2)
    Z, Y = experts // X, lanes // CORES
    rows, model_width = expert_batch_tokens.shape
    seq, kw = queries.shape
    vw = stream_content_vectors.shape[1]
    width = shared_gate_matrix.shape[1]
    chunks = seq // rows
    stages = (Z - 1) * CH
    units = 3 + stages + chunks
    tile = min(256, width)
    tiles = width // tile
    args = (
        queries,
        sequence_keys,
        stream_content_vectors,
        output_gate_logits,
        retention_preactivation,
        additional_fade_bias,
        attention_group_rescale.reshape(1, DV),
        output_projection,
        expert_batch_tokens,
        expert_norm_gain.reshape(1, model_width),
        routed_expert_index.T,
        routed_expert_weights.T,
        expert_gate_matrix[0],
        expert_up_matrix[0],
        expert_down_matrix[0],
        shared_gate_matrix,
        shared_up_matrix,
        shared_down_matrix,
    )
    outs = (
        jax.ShapeDtypeStruct((seq, output_projection.shape[1]), bf16),
        jax.ShapeDtypeStruct((rows, shared_down_matrix.shape[1]), bf16),
    )
    dma = lambda *shape: pltpu.SemaphoreType.DMA(shape)
    scratch = [pltpu.VMEM(a.shape, a.dtype) for a in args]
    scratch += [
        pltpu.VMEM((experts, CH, CORES, rows // (CH * CORES), model_width), bf16),
        pltpu.VMEM((2, lanes, tiles, rows, tile), bf16),
        pltpu.VMEM((stages, lanes, tiles, X * rows // CH, tile), bf16),
        pltpu.VMEM((1, lanes, tiles, (X - 1) * rows, tile), bf16),
        pltpu.VMEM((chunks, lanes, tiles, rows, tile), bf16),
        pltpu.VMEM((experts, CH, rows // CH, outs[1].shape[1]), bf16),
        pltpu.VMEM((experts, CH, rows // CH, outs[1].shape[1]), bf16),
        pltpu.VMEM((X, DV + PAD, kw), bf16),
        pltpu.VMEM((2, DV, kw), bf16),
        pltpu.VMEM((seq, vw), f32),
        pltpu.VMEM((seq, kw), bf16),
        pltpu.VMEM((DV + 8, kw), f32),
        pltpu.VMEM((DV, kw), f32),
        pltpu.VMEM((rows, outs[1].shape[1]), f32),
        dma(11),
        dma(2 + (X - 1) * (Z + 2), CH),
        dma(Z, CH),
        dma(CH),
        dma(X - 1, Z, CH),
        dma(X - 1, 2, CH),
        dma(experts, CH),
        dma(experts, CH),
        dma(5),
        dma(units),
        dma(Y - 1, 10),
        dma(Y - 1, (3 + stages) * tiles + chunks),
        dma(Y - 1, 3),
        dma(Y - 1, units),
        dma(10),
        dma(experts),
        dma(X - 1),
        dma(X - 1),
        dma(1),
        dma(1),
    ]
    made = pl.pallas_call(
        functools.partial(body, (Z, X, Y)),
        out_shape=tuple(pltpu.VMEM(o.shape, o.dtype) for o in outs),
        in_specs=[pl.BlockSpec(memory_space=pl.ANY)] * len(args),
        out_specs=tuple([pl.BlockSpec(memory_space=pltpu.VMEM)] * len(outs)),
        scratch_shapes=scratch,
        compiler_params=pltpu.CompilerParams(
            collective_id=0, has_side_effects=True, vmem_limit_bytes=66000000
        ),
        cost_estimate=pl.CostEstimate(
            flops=10**10, bytes_accessed=20 * 2**20, transcendentals=10**6
        ),
        name="step",
    )(*args)
    return pl.pallas_call(
        settle,
        out_shape=outs,
        in_specs=[pl.BlockSpec(memory_space=pltpu.VMEM)] * 2,
        out_specs=tuple([pl.BlockSpec(memory_space=pl.ANY)] * 2),
        scratch_shapes=[dma(2)],
        cost_estimate=pl.CostEstimate(flops=10**6, bytes_accessed=2**21, transcendentals=0),
        name="settle",
    )(*[pltpu.with_memory_space_constraint(m, pltpu.VMEM) for m in made])


def settle(mixer_ref, blend_ref, mixer_out, blend_out, sem):
    writes = [
        pltpu.make_async_copy(mixer_ref, mixer_out, sem.at[0]),
        pltpu.make_async_copy(blend_ref, blend_out, sem.at[1]),
    ]
    for copy in writes:
        copy.start()
    for copy in writes:
        copy.wait()


def solution(mesh):
    in_specs = (
        P("ep", "tp"),
        P("ep", "tp"),
        P("ep", "tp"),
        P("ep", "tp"),
        P("ep", "tp"),
        P("ep", "tp"),
        P(),
        P(None, "tp"),
        P("ep", None),
        P(),
        P("ep", None),
        P("ep", None),
        P("ep", None, "tp"),
        P("ep", None, "tp"),
        P("ep", None, "tp"),
        P(None, "tp"),
        P(None, "tp"),
        P(None, "tp"),
    )
    out_specs = (P("ep", "tp"), P("ep", "tp"))
    return jax.shard_map(local, mesh=mesh, in_specs=in_specs, out_specs=out_specs, check_vma=False)
```
